32 devices in a mesh: sp: 16 (over z, y, x), tp: 2 (over core).
Axes of the slice: x: 2, y: 2, z: 4, core: 2. Of those that a mesh axis runs over, the one named last changes fastest.
Arguments:
- tokens: bfloat16 [4096, 2048], P(('sp', 'tp')), may hold values from -6 to 6
- mix_gain: float32 [2048], replicated, may hold values from 0.1 to 1.9
- query_proj: bfloat16 [2048, 1536], P(None, 'tp'), may hold values from -4 to 4
- compressed_projection: bfloat16 [2048, 256], replicated, may hold values from -0.125 to 0.125
- compressed_norm_gain: float32 [256], replicated, may hold values from 0.1 to 1.9
- rope_proj: bfloat16 [2048, 64], replicated, may hold values from -0.125 to 0.125
- key_up: bfloat16 [256, 1024], P(None, 'tp'), may hold values from -4 to 4
- value_up_weight: bfloat16 [256, 1024], P(None, 'tp'), may hold values from -0.375 to 0.375
- scan_input: bfloat16 [2048, 2048], P('sp', 'tp'), may hold values from -0.125 to 0.125
- scan_gate: bfloat16 [2048, 2048], P('sp', 'tp'), may hold values from -0.125 to 0.125
- scan_write: bfloat16 [2048, 1024], P('sp', 'tp'), may hold values from -0.125 to 0.125
- scan_read: bfloat16 [2048, 1024], P('sp', 'tp'), may hold values from -0.125 to 0.125
- step_proj: bfloat16 [2048, 32], replicated, may hold values from -0.125 to 0.125
- conv_input: bfloat16 [4, 2048], P(None, 'tp'), may hold values from -3 to 3
- conv_write: bfloat16 [4, 1024], P(None, 'tp'), may hold values from -3 to 3
- conv_read: bfloat16 [4, 1024], P(None, 'tp'), may hold values from -3 to 3
- decay_log: float32 [32], P('tp'), may hold values from -16 to -2.8
- decay_offset: float32 [4096, 32], P('sp', 'tp'), may hold values from -2.2 to 0
- skip_gain: float32 [32], P('tp'), may hold values from 0.1 to 1.9
- group_gain: float32 [2048], P('tp'), may hold values from 0.1 to 1.9
Outputs:
- attended: bfloat16 [4096, 1024], P('sp', 'tp')
- scanned: bfloat16 [4096, 2048], P('sp', 'tp')
The draws below stay inside these ranges and needn't reach their ends.
All inputs are finite; a program needn't handle non-finite values.
Results may differ from the reference program's by a relative error of at most 0.017.
The reference program's roundings to bfloat16 on the way count: a program that leaves them out, or rounds other values in their place, can miss the bound.
Values may be sent and summed in bfloat16 or wider, within the bound.
No kernel may reach another device: no remote copies, remote signals or barrier semaphores. Data moves between devices by JAX's collectives and lax.ppermute only.
A program may use at most 128 MiB of HBM per device.

```python
import jax
import jax.numpy as jnp
from jax import lax

MODEL_WIDTH = 2048
ATTENTION_HEADS = 8
UNROTATED_WIDTH = 128
ROPE = 64
VALUE_WIDTH = 128
LATENT_KEY_WIDTH = 256
SSM_HEADS = 32
SSM_DIM = 64
SSM_GROUPS = 8
SSM_STATE = 128
CONV = 4
BLOCK = 128
TOK_DEV = 256
SEQ = 4096


def draw_decay_log(key, part):
    pick_key, fast_key, slow_key = jax.random.split(jax.random.fold_in(key, 11), 3)
    fast = jax.random.uniform(pick_key, (SSM_HEADS,), jnp.float32) < 0.5
    fast_rate = jnp.exp(jax.random.uniform(fast_key, (SSM_HEADS,), jnp.float32, jnp.log(0.02), jnp.log(0.06)))
    slow_rate = jnp.exp(jax.random.uniform(slow_key, (SSM_HEADS,), jnp.float32, jnp.log(0.05), jnp.log(0.3))) / SEQ
    return jnp.log(jnp.where(fast, fast_rate, slow_rate)).astype(jnp.float32)


def draw_decay_offset(key, part):
    rate_key, place_key, depth_key = jax.random.split(jax.random.fold_in(key, 23), 3)
    blocks = SEQ // TOK_DEV
    rates = jnp.exp(jax.random.uniform(rate_key, (blocks, SSM_HEADS), jnp.float32, jnp.log(0.1), jnp.log(0.6)))
    reference_amount = -jnp.repeat(rates, TOK_DEV, axis=0) / SEQ
    places = jax.random.randint(place_key, (3,), 0, SEQ)
    layer_tiers = jnp.log(jax.random.uniform(depth_key, (3,), jnp.float32, 0.5, 0.8))
    match_flags = (jnp.arange(SEQ)[:, None] == places[None, :]).astype(jnp.float32)
    sudden_outlier = jnp.dot(match_flags, layer_tiers)[:, None]
    return (reference_amount + sudden_outlier).astype(jnp.float32)


def shared_direction(key):
    order_key, strength_key, direction_key = jax.random.split(jax.random.fold_in(key, 37), 3)
    chosen = (jax.random.permutation(order_key, ATTENTION_HEADS) < ATTENTION_HEADS // 2).astype(jnp.float32)
    strength = jnp.exp(jax.random.uniform(strength_key, (ATTENTION_HEADS,), jnp.float32, jnp.log(6.0), jnp.log(18.0)))
    direction = jax.random.normal(direction_key, (ATTENTION_HEADS, UNROTATED_WIDTH), jnp.float32)
    direction = direction / jnp.sqrt(jnp.sum(direction * direction, axis=1, keepdims=True))
    magnitude = jnp.sqrt(strength * jnp.sqrt(jnp.float32(UNROTATED_WIDTH + ROPE)))
    return direction * (magnitude * chosen)[:, None]


def draw_query_proj(key, part):
    planted = shared_direction(key)
    noise_random_key, along_sequence_key = jax.random.split(jax.random.fold_in(key, 41))
    reference_amount = jnp.clip(jax.random.normal(noise_random_key, (MODEL_WIDTH, ATTENTION_HEADS * (UNROTATED_WIDTH + ROPE)), jnp.float32), -6.0, 6.0) / jnp.sqrt(jnp.float32(MODEL_WIDTH))
    along_sequence = jax.random.normal(along_sequence_key, (MODEL_WIDTH,), jnp.float32)
    along_sequence = along_sequence / jnp.sqrt(jnp.sum(along_sequence * along_sequence))
    padded = jnp.concatenate([planted, jnp.zeros((ATTENTION_HEADS, ROPE), jnp.float32)], axis=1).reshape(ATTENTION_HEADS * (UNROTATED_WIDTH + ROPE))
    return jnp.clip(reference_amount + along_sequence[:, None] * padded[None, :], -4.0, 4.0).astype(jnp.bfloat16)


def draw_key_up(key, part):
    planted = shared_direction(key)
    noise_random_key, along_sequence_key = jax.random.split(jax.random.fold_in(key, 43))
    reference_amount = jnp.clip(jax.random.normal(noise_random_key, (LATENT_KEY_WIDTH, ATTENTION_HEADS * UNROTATED_WIDTH), jnp.float32), -6.0, 6.0) / jnp.sqrt(jnp.float32(LATENT_KEY_WIDTH))
    along_sequence = jax.random.normal(along_sequence_key, (LATENT_KEY_WIDTH,), jnp.float32)
    along_sequence = along_sequence / jnp.sqrt(jnp.sum(along_sequence * along_sequence))
    flat = planted.reshape(ATTENTION_HEADS * UNROTATED_WIDTH)
    return jnp.clip(reference_amount + along_sequence[:, None] * flat[None, :], -4.0, 4.0).astype(jnp.bfloat16)


def levels(own_key, shape, cuts, low, top_value):
    def one(dim, shards_of):
        draws = jax.random.uniform(jax.random.fold_in(jax.random.fold_in(own_key, 6), dim), (shards_of,), jnp.float32, low / len(cuts), top_value / len(cuts))
        return jnp.repeat(jnp.exp(draws), shape[dim] // shards_of).reshape((-1,) + (1,) * (len(shape) - dim - 1))

    level = one(*cuts[0])
    for cut in cuts[1:]:
        level = level * one(*cut)
    return level


def gaussian(own_key, extent, deviation, bound, shards=(), kind=jnp.bfloat16):
    drawn = jax.random.normal(own_key, extent, jnp.float32) * deviation
    if len(shards) > 0:
        drawn = levels(own_key, extent, shards, -0.22, 0.18) * drawn
    return jnp.clip(drawn, min=-bound, max=bound).astype(kind)


def setup_inputs(seed: int = 0) -> dict:
    seeds = jax.random.split(jax.random.key(seed), 21)
    return {
        "tokens": gaussian(seeds[0], (SEQ, MODEL_WIDTH), 1.0, 6.0, ((0, 32),)),
        "mix_gain": jnp.clip(1.0 + 0.18 * jax.random.normal(seeds[1], (MODEL_WIDTH,), jnp.float32), 0.1, 1.9),
        "query_proj": draw_query_proj(jax.random.fold_in(seeds[20], 71), 0),
        "compressed_projection": gaussian(seeds[3], (MODEL_WIDTH, LATENT_KEY_WIDTH), MODEL_WIDTH ** -0.5, 0.125),
        "compressed_norm_gain": jnp.clip(1.0 + 0.18 * jax.random.normal(seeds[4], (LATENT_KEY_WIDTH,), jnp.float32), 0.1, 1.9),
        "rope_proj": gaussian(seeds[5], (MODEL_WIDTH, ROPE), MODEL_WIDTH ** -0.5, 0.125),
        "key_up": draw_key_up(jax.random.fold_in(seeds[20], 71), 0),
        "value_up_weight": gaussian(seeds[7], (LATENT_KEY_WIDTH, ATTENTION_HEADS * VALUE_WIDTH), LATENT_KEY_WIDTH ** -0.5, 0.375, ((1, 2),)),
        "scan_input": gaussian(seeds[8], (MODEL_WIDTH, SSM_HEADS * SSM_DIM), MODEL_WIDTH ** -0.5, 0.125, ((0, 16), (1, 2))),
        "scan_gate": gaussian(seeds[9], (MODEL_WIDTH, SSM_HEADS * SSM_DIM), MODEL_WIDTH ** -0.5, 0.125, ((0, 16), (1, 2))),
        "scan_write": gaussian(seeds[10], (MODEL_WIDTH, SSM_GROUPS * SSM_STATE), MODEL_WIDTH ** -0.5, 0.125, ((0, 16), (1, 2))),
        "scan_read": gaussian(seeds[11], (MODEL_WIDTH, SSM_GROUPS * SSM_STATE), MODEL_WIDTH ** -0.5, 0.125, ((0, 16), (1, 2))),
        "step_proj": gaussian(seeds[12], (MODEL_WIDTH, SSM_HEADS), MODEL_WIDTH ** -0.5, 0.125),
        "conv_input": gaussian(seeds[13], (CONV, SSM_HEADS * SSM_DIM), CONV ** -0.5, 3.0, ((1, 2),)),
        "conv_write": gaussian(seeds[14], (CONV, SSM_GROUPS * SSM_STATE), CONV ** -0.5, 3.0, ((1, 2),)),
        "conv_read": gaussian(seeds[15], (CONV, SSM_GROUPS * SSM_STATE), CONV ** -0.5, 3.0, ((1, 2),)),
        "decay_log": draw_decay_log(jax.random.fold_in(seeds[20], 71), 0),
        "decay_offset": draw_decay_offset(jax.random.fold_in(seeds[20], 71), 0),
        "skip_gain": jnp.clip(1.0 + 0.18 * jax.random.normal(seeds[18], (SSM_HEADS,), jnp.float32), 0.1, 1.9),
        "group_gain": jnp.clip(1.0 + 0.18 * jax.random.normal(seeds[19], (SSM_HEADS * SSM_DIM,), jnp.float32), 0.1, 1.9),
    }


eps = 1e-06
theta = 10000.0
floor_score = -1e+30

def rms_scale(values, gain):
    wide = values.astype(jnp.float32)
    return wide * lax.rsqrt(lax.optimization_barrier(jnp.mean(wide * wide, axis=-1, keepdims=True)) + eps) * gain

def rotate(values, positions):
    half = values.shape[-1] // 2
    freqs = theta ** (-jnp.arange(half, dtype=jnp.float32) * 2.0 / values.shape[-1])
    angle = positions.astype(jnp.float32)[:, None] * freqs[None, :]
    cosine = jnp.cos(angle)
    sine = jnp.sin(angle)
    if values.ndim == 3:
        cosine = cosine[:, None, :]
        sine = sine[:, None, :]
    first = values[..., :half]
    second = values[..., half:]
    return jnp.concatenate([first * cosine - second * sine, second * cosine + first * sine], axis=-1)

def short_conv(values, edge, taps):
    span = taps.shape[0]
    length = values.shape[0]
    padded = jnp.concatenate([edge, values], axis=0).astype(jnp.float32)
    result = jnp.zeros(values.shape, jnp.float32)
    for index in range(span):
        result = result + taps[index].astype(jnp.float32)[None, :] * padded[index:index + length]
    return jax.nn.silu(result).astype(jnp.bfloat16)

def blockwise_scan(heads, steps, decays, writes, reads, state, block):
    count = heads.shape[0] // block
    best = lax.Precision.HIGHEST

    def split(values):
        return values.reshape((count, block) + values.shape[1:])

    def one_block(state, inputs):
        head_block, step_block, decay_block, write_block, read_block = inputs
        running = jnp.cumsum(decay_block, axis=0)
        causal = jnp.tril(jnp.ones((block, block), dtype=bool))[:, :, None, None]
        spread = running[:, None] - running[None, :]
        fading = jnp.where(causal, jnp.exp(jnp.where(causal, spread, 0.0)), 0.0)
        inner = jnp.einsum('lgn,sgn->lsg', read_block, write_block, precision=best)
        mixing = inner[..., None] * fading * step_block[None]
        within = jnp.einsum('lsgr,sgrp->lgrp', mixing, head_block, precision=best)
        carried = jnp.einsum('lgn,grpn->lgrp', read_block, state, precision=best) * jnp.exp(running)[..., None]
        to_end = jnp.exp(running[-1:] - running) * step_block
        update = jnp.einsum('sgn,sgr,sgrp->grpn', write_block, to_end, head_block, precision=best)
        state = jnp.exp(running[-1])[..., None, None] * state + update
        return (state, within + carried)
    state, outputs = lax.scan(one_block, state, (split(heads), split(steps), split(decays), split(writes), split(reads)))
    return (state, outputs.reshape(heads.shape))

def gated_norm(mixed, gate, gain):
    length = mixed.shape[0]
    groups = mixed.shape[1]
    flat = mixed.reshape(length, groups, -1)
    gated = flat * jax.nn.silu(gate.astype(jnp.float32)).reshape(length, groups, -1)
    scaled = gated * lax.rsqrt(lax.optimization_barrier(jnp.mean(gated * gated, axis=-1, keepdims=True)) + eps)
    return (scaled * gain.reshape(groups, -1)[None]).reshape(length, -1).astype(jnp.bfloat16)

def reference(tokens, mix_gain, query_proj, compressed_projection, compressed_norm_gain, rope_proj, key_up, value_up_weight, scan_input, scan_gate, scan_write, scan_read, step_proj, conv_input, conv_write, conv_read, decay_log, decay_offset, skip_gain, group_gain):
    positions = jnp.arange(SEQ, dtype=jnp.int32)
    normed = rms_scale(tokens, mix_gain).astype(jnp.bfloat16)
    query = jnp.dot(normed, query_proj, preferred_element_type=jnp.float32).astype(jnp.bfloat16)
    query = query.reshape(SEQ, ATTENTION_HEADS, UNROTATED_WIDTH + ROPE)
    query_plain = query[:, :, :UNROTATED_WIDTH]
    query_turned = rotate(query[:, :, UNROTATED_WIDTH:].astype(jnp.float32), positions).astype(jnp.bfloat16)
    latent = rms_scale(jnp.dot(normed, compressed_projection, preferred_element_type=jnp.float32), compressed_norm_gain).astype(jnp.bfloat16)
    key_turned = rotate(jnp.dot(normed, rope_proj, preferred_element_type=jnp.float32), positions).astype(jnp.bfloat16)
    key_plain = jnp.dot(latent, key_up, preferred_element_type=jnp.float32).astype(jnp.bfloat16).reshape(SEQ, ATTENTION_HEADS, UNROTATED_WIDTH)
    values = jnp.dot(latent, value_up_weight, preferred_element_type=jnp.float32).astype(jnp.bfloat16).reshape(SEQ, ATTENTION_HEADS, VALUE_WIDTH)
    scale = (UNROTATED_WIDTH + ROPE) ** (-0.5)

    def one_query_block(index):
        start = index * TOK_DEV
        q_plain = lax.dynamic_slice_in_dim(query_plain, start, TOK_DEV, 0).astype(jnp.float32)
        q_turned = lax.dynamic_slice_in_dim(query_turned, start, TOK_DEV, 0).astype(jnp.float32)
        q_positions = start + jnp.arange(TOK_DEV, dtype=jnp.int32)

        def visit(step, carry):
            highest, total, summed = carry
            k_start = step * TOK_DEV
            k_plain = lax.dynamic_slice_in_dim(key_plain, k_start, TOK_DEV, 0).astype(jnp.float32)
            k_turned = lax.dynamic_slice_in_dim(key_turned, k_start, TOK_DEV, 0).astype(jnp.float32)
            k_values = lax.dynamic_slice_in_dim(values, k_start, TOK_DEV, 0).astype(jnp.float32)
            k_positions = k_start + jnp.arange(TOK_DEV, dtype=jnp.int32)
            scores = jnp.einsum('qhd,khd->hqk', q_plain, k_plain) + jnp.einsum('qhd,kd->hqk', q_turned, k_turned)
            scores = scores * scale
            scores = jnp.where(k_positions[None, None, :] <= q_positions[None, :, None], scores, -jnp.inf)
            new_highest = jnp.maximum(highest, lax.optimization_barrier(jnp.max(scores, axis=-1)))
            weights = jnp.exp(scores - new_highest[..., None])
            shrink = jnp.exp(highest - new_highest)
            total = total * shrink + lax.optimization_barrier(jnp.sum(weights, axis=-1))
            rounded = lax.optimization_barrier(weights.astype(jnp.bfloat16)).astype(jnp.float32)
            summed = summed * shrink[..., None] + jnp.einsum('hqk,khd->hqd', rounded, k_values)
            return (new_highest, total, summed)
        initial_recurrent = (jnp.full((ATTENTION_HEADS, TOK_DEV), floor_score, jnp.float32), jnp.zeros((ATTENTION_HEADS, TOK_DEV), jnp.float32), jnp.zeros((ATTENTION_HEADS, TOK_DEV, VALUE_WIDTH), jnp.float32))
        highest, total, summed = lax.fori_loop(0, index + 1, visit, initial_recurrent)
        return (summed / total[..., None]).astype(jnp.bfloat16)
    blocks = lax.map(one_query_block, jnp.arange(SEQ // TOK_DEV, dtype=jnp.int32))
    attended = jnp.transpose(blocks, (0, 2, 1, 3)).reshape(SEQ, ATTENTION_HEADS * VALUE_WIDTH)
    groups = SSM_GROUPS
    per_group = SSM_HEADS // SSM_GROUPS
    head_raw = jnp.dot(normed, scan_input, preferred_element_type=jnp.float32).astype(jnp.bfloat16)
    gate = jnp.dot(normed, scan_gate, preferred_element_type=jnp.float32).astype(jnp.bfloat16)
    write_raw = jnp.dot(normed, scan_write, preferred_element_type=jnp.float32).astype(jnp.bfloat16)
    read_raw = jnp.dot(normed, scan_read, preferred_element_type=jnp.float32).astype(jnp.bfloat16)
    step_size = jax.nn.softplus(jnp.dot(normed, step_proj, preferred_element_type=jnp.float32))
    heads = short_conv(head_raw, jnp.zeros((CONV - 1, head_raw.shape[1]), jnp.bfloat16), conv_input)
    writes = short_conv(write_raw, jnp.zeros((CONV - 1, write_raw.shape[1]), jnp.bfloat16), conv_write)
    reads = short_conv(read_raw, jnp.zeros((CONV - 1, read_raw.shape[1]), jnp.bfloat16), conv_read)
    log_decay = -jnp.exp(decay_log)[None, :] * step_size + decay_offset
    head_values = heads.astype(jnp.float32).reshape(SEQ, groups, per_group, SSM_DIM)
    step_values = step_size.reshape(SEQ, groups, per_group)
    decay_values = log_decay.reshape(SEQ, groups, per_group)
    write_values = writes.astype(jnp.float32).reshape(SEQ, groups, SSM_STATE)
    output_entries = reads.astype(jnp.float32).reshape(SEQ, groups, SSM_STATE)
    empty_state = jnp.zeros((groups, per_group, SSM_DIM, SSM_STATE), jnp.float32)
    final_state, mixed = blockwise_scan(head_values, step_values, decay_values, write_values, output_entries, empty_state, BLOCK)
    mixed = mixed + skip_gain.reshape(groups, per_group)[None, :, :, None] * head_values
    scanned = gated_norm(mixed, gate, group_gain)
    return (attended, scanned)
```

```python
import functools
import math

import jax
import jax.numpy as jnp
from jax import lax
from jax.experimental import pallas as pl
from jax.experimental.pallas import tpu as pltpu
from jax.sharding import Mesh
from jax.sharding import PartitionSpec as P

UNROTATED_WIDTH = 128
ROPE = 64
VALUE_WIDTH = 128
SSM_DIM = 64
SSM_STATE = 128

eps = 1e-06
theta = 10000.0
floor_score = -1e30
LANES = 128
DIRECT = 8


f32 = jnp.float32
bf16 = jnp.bfloat16


def vmem():
    return pl.BlockSpec(memory_space=pltpu.VMEM)


def smem():
    return pl.BlockSpec(memory_space=pltpu.SMEM)


def hbm():
    return pl.BlockSpec(memory_space=pl.ANY)


def nt(a, b):
    return lax.dot_general(a, b, (((1,), (1,)), ((), ())), preferred_element_type=f32)


def tn(a, b):
    return lax.dot_general(a, b, (((0,), (0,)), ((), ())), preferred_element_type=f32)


def nn(a, b, precision=None):
    return lax.dot_general(
        a, b, (((1,), (0,)), ((), ())), precision=precision, preferred_element_type=f32
    )


def exchange(value, axis):
    count = lax.axis_size(axis)
    if count == 1:
        return [value]
    if count <= DIRECT and count & (count - 1) == 0:
        pieces = [value]
        for k in range(1, count):
            pieces.append(lax.ppermute(value, axis, [(i, i ^ k) for i in range(count)]))
        return pieces
    everything = lax.all_gather(value, axis)
    here = lax.axis_index(axis)
    assert count & (count - 1) == 0
    return [
        lax.dynamic_index_in_dim(everything, here ^ k, 0, keepdims=False) for k in range(count)
    ]


def ring(value, axis):
    count = lax.axis_size(axis)
    if count <= DIRECT:
        pieces = [value]
        for _ in range(1, count):
            pieces.append(
                lax.ppermute(pieces[-1], axis, [(i, (i + 1) % count) for i in range(count)])
            )
        return pieces
    everything = lax.all_gather(value, axis)
    here = lax.axis_index(axis)
    return [
        lax.dynamic_index_in_dim(everything, (here - k) % count, 0, keepdims=False)
        for k in range(count)
    ]


def spread_last(value, axis):
    count = lax.axis_size(axis)
    step = 1
    while step < count:
        pairs = [
            (count - 1 - j, count - 1 - j - step) for j in range(step) if count - 1 - j - step >= 0
        ]
        value = value + lax.ppermute(value, axis, pairs)
        step *= 2
    return value


def norm_kernel(tokens_ref, gain_ref, out_ref):
    wide = tokens_ref[...].astype(f32)
    scale = lax.rsqrt(jnp.mean(wide * wide, axis=-1, keepdims=True) + eps)
    out_ref[...] = (wide * scale * gain_ref[...]).astype(bf16)


def latent_kernel(x_ref, proj_ref, gain_ref, rope_ref, cos_ref, sin_ref, out_ref):
    x = x_ref[...]
    wide = nn(x, proj_ref[...])
    scale = lax.rsqrt(jnp.mean(wide * wide, axis=-1, keepdims=True) + eps)
    width = wide.shape[1]
    out_ref[:, :width] = (wide * scale * gain_ref[...]).astype(bf16)
    turn = nn(x, rope_ref[...])
    rope = turn.shape[1]
    half = rope // 2
    row = lax.broadcasted_iota(jnp.int32, (rope, 2 * rope), 0)
    col = lax.broadcasted_iota(jnp.int32, (rope, 2 * rope), 1) % rope
    same = (row == col).astype(f32)
    swap = (row == (col + half) % rope).astype(f32)
    best = lax.Precision.HIGHEST
    turned = nn(turn, same, best) * cos_ref[...] + nn(turn, swap, best) * sin_ref[...]
    out_ref[:, width:] = turned.astype(bf16)


def query_kernel(order_ref, *refs, count, heads):
    pieces = refs[:count]
    w_ref, cos_ref, sin_ref, plain_ref, turned_ref = refs[count:]
    rows = pieces[0].shape[0]
    w = w_ref[...]
    lane = lax.broadcasted_iota(jnp.int32, (rows, LANES), 1)
    low = lane < ROPE
    first = lane % ROPE < ROPE // 2
    for k in range(count):
        start = pl.multiple_of(order_ref[k] * rows, rows)
        here = pl.ds(start, rows)
        q = nn(pieces[k][...], w).astype(bf16).astype(f32)
        cos = cos_ref[here, :]
        sin = sin_ref[here, :]
        for pair in range(heads // 2):
            base = pair * 3 * LANES
            t0 = q[:, base : base + LANES]
            t1 = q[:, base + LANES : base + 2 * LANES]
            t2 = q[:, base + 2 * LANES : base + 3 * LANES]
            odd = jnp.where(low, pltpu.roll(t1, ROPE, 1), pltpu.roll(t2, ROPE, 1))
            turn = jnp.where(low, t1, t2)
            other = jnp.where(
                first, pltpu.roll(turn, LANES - ROPE // 2, 1), pltpu.roll(turn, ROPE // 2, 1)
            )
            turned = turn * cos + other * sin
            at = pair * 2 * LANES
            plain_ref[here, at : at + LANES] = t0.astype(bf16)
            plain_ref[here, at + LANES : at + 2 * LANES] = odd.astype(bf16)
            turned_ref[here, pair * LANES : (pair + 1) * LANES] = turned.astype(bf16)


def attention_kernel(
    order_ref, plain_ref, turned_ref, ku_ref, vu_ref, *refs, arrays, slots, heads, blocks
):
    pieces = refs[:arrays]
    out_ref = refs[arrays]
    keys, q_s, top_s, sum_s, acc_s, sems = refs[arrays + 1 :]
    length = plain_ref.shape[0]
    rows = pieces[0].shape[1]
    per_block = length // rows
    width = ku_ref.shape[0]
    here = order_ref[arrays * slots]
    factor = (UNROTATED_WIDTH + ROPE) ** -0.5 * math.log2(math.e)

    def copy_into(array, slot, place):
        start = pl.multiple_of(place * rows, rows)
        return pltpu.make_async_copy(
            pieces[array].at[slot], keys.at[pl.ds(start, rows), :], sems.at[place]
        )

    for array in range(arrays):
        for slot in range(slots):
            place = order_ref[array * slots + slot]

            @pl.when(place < (here + 1) * per_block)
            def _():
                copy_into(array, slot, place).start()

    lane = lax.broadcasted_iota(jnp.int32, (length, LANES), 1)
    for h in range(heads):
        q_s[h, :, :LANES] = plain_ref[:, h * LANES : (h + 1) * LANES]
        turned = turned_ref[:, (h // 2) * LANES : (h // 2 + 1) * LANES]
        keep = lane < ROPE if h % 2 == 0 else lane >= ROPE
        q_s[h, :, LANES:] = jnp.where(keep, turned, jnp.zeros_like(turned))
    top_s[...] = jnp.full(top_s.shape, floor_score, f32)
    sum_s[...] = jnp.zeros(sum_s.shape, f32)
    acc_s[...] = jnp.zeros(acc_s.shape, f32)

    def visit(block, masked):
        for part in range(per_block):
            copy_into(0, 0, block * per_block + part).wait()
        at = pl.ds(pl.multiple_of(block * length, length), length)
        latent = keys[at, :width]
        shared = keys[at, width:]
        key_plain = nn(latent, ku_ref[...]).astype(bf16)
        values = nt(vu_ref[...], latent).astype(bf16)
        if masked:
            key_at = lax.broadcasted_iota(jnp.int32, (length, length), 0)
            query_at = lax.broadcasted_iota(jnp.int32, (length, length), 1)
            seen = key_at <= query_at
        for h in range(heads):
            key = jnp.concatenate([key_plain[:, h * LANES : (h + 1) * LANES], shared], axis=1)
            score = nt(key, q_s[h])
            if masked:
                score = jnp.where(seen, score, -jnp.inf)
            old = top_s[h]
            top = jnp.maximum(old, jnp.max(score, axis=0, keepdims=True))
            weight = jnp.exp2((score - top) * factor)
            shrink = jnp.exp2((old - top) * factor)
            top_s[h] = top
            sum_s[h] = sum_s[h] * shrink + jnp.sum(weight, axis=0, keepdims=True)
            acc_s[h] = acc_s[h] * shrink + nn(
                values[h * VALUE_WIDTH : (h + 1) * VALUE_WIDTH, :], weight.astype(bf16)
            )

    def body(block, carry):
        visit(block, False)
        return carry

    lax.fori_loop(0, here, body, 0)
    visit(here, True)
    for h in range(heads):
        result = (acc_s[h] / sum_s[h]).T
        out_ref[:, h * VALUE_WIDTH : (h + 1) * VALUE_WIDTH] = result.astype(bf16)


def wide_heads(values, heads, lane):
    tiles = []
    for pair in range(0, heads, 2):
        a = jnp.broadcast_to(values[:, pair : pair + 1], (values.shape[0], LANES))
        b = jnp.broadcast_to(values[:, pair + 1 : pair + 2], (values.shape[0], LANES))
        tiles.append(jnp.where(lane < SSM_DIM, a, b))
    return jnp.concatenate(tiles, axis=1)


def scan_kernel(
    xorder_ref,
    worder_ref,
    *refs,
    planes,
    cores,
    weights,
    length,
    heads,
):
    nx = planes * cores
    xs_in = refs[:nx]
    ws_in = refs[nx : nx + weights]
    (
        halo_ref,
        step_ref,
        taps_ref,
        rate_ref,
        offset_ref,
        skip_ref,
        mixed_ref,
        reads_ref,
        gate_ref,
        run_ref,
        state_ref,
        xs,
        ws,
        pad,
        state_s,
        base_s,
        xsem,
        wsem,
    ) = refs[nx + weights :]
    rows = xs_in[0].shape[0]
    depth = ws_in[0].shape[0]
    channels = heads * SSM_DIM
    conv = channels + 2 * SSM_STATE

    for k in range(weights):
        start = pl.multiple_of(worder_ref[k] * depth, depth)
        pltpu.make_async_copy(ws_in[k], ws.at[pl.ds(start, depth), :], wsem.at[k]).start()
    for k in range(nx):
        place = xorder_ref[k]
        start = pl.multiple_of(place * rows, rows)
        pltpu.make_async_copy(xs_in[k], xs.at[pl.ds(start, rows), :], xsem.at[place]).start()
    state_s[...] = jnp.zeros(state_s.shape, f32)
    base_s[...] = jnp.zeros(base_s.shape, f32)
    for k in range(weights):
        start = pl.multiple_of(worder_ref[k] * depth, depth)
        pltpu.make_async_copy(ws_in[k], ws.at[pl.ds(start, depth), :], wsem.at[k]).wait()
    pad[0:8, :] = nn(halo_ref[...], ws[:, :conv]).astype(bf16).astype(f32)

    lane = lax.broadcasted_iota(jnp.int32, (length, LANES), 1)
    li = lax.broadcasted_iota(jnp.int32, (length, length), 0)
    si = lax.broadcasted_iota(jnp.int32, (length, length), 1)
    causal = si <= li
    tril = causal.astype(f32)
    wide_lane = lax.broadcasted_iota(jnp.int32, (length, channels), 1)
    span = taps_ref.shape[0]

    def chunk(c, carry):
        for t in range(cores):
            place = c * cores + t
            start = pl.multiple_of(place * rows, rows)
            pltpu.make_async_copy(
                xs_in[0], xs.at[pl.ds(start, rows), :], xsem.at[place]
            ).wait()
        here = pl.ds(pl.multiple_of(c * length, length), length)
        x = xs[here, :]
        raw = nn(x, ws[...]).astype(bf16)
        gate_ref[here, :] = raw[:, conv:]
        pad[8:, :] = raw[:, :conv].astype(f32)
        total = jnp.zeros((length, conv), f32)
        for k in range(span):
            total = total + taps_ref[k : k + 1, :] * pad[8 - span + 1 + k : 8 - span + 1 + k + length, :]
        mixed_in = jax.nn.silu(total).astype(bf16)
        pad[0:8, :] = pad[length : length + 8, :]
        head = mixed_in[:, :channels].astype(f32)
        write = mixed_in[:, channels : channels + SSM_STATE]
        read = mixed_in[:, channels + SSM_STATE :]
        reads_ref[here, :] = read
        step = jax.nn.softplus(nn(x, step_ref[...]))
        decay = rate_ref[...] * step + offset_ref[here, :]
        running = nn(tril, decay, lax.Precision.HIGHEST)
        run_ref[here, :] = running + base_s[...]
        base_s[...] = base_s[...] + running[length - 1 :, :]
        across = running.T
        stepped = head * wide_heads(step, heads, lane)
        inner = nt(read, write)
        reach = jnp.exp(wide_heads(running, heads, lane))
        out = nn(read, state_s[...].astype(bf16)) * reach + skip_ref[...] * head
        for h in range(heads):
            spread = running[:, h : h + 1] - across[h : h + 1, :]
            fading = jnp.exp(jnp.where(causal, spread, floor_score))
            mine = (wide_lane >= h * SSM_DIM) & (wide_lane < (h + 1) * SSM_DIM)
            out = out + nn(
                (inner * fading).astype(bf16), jnp.where(mine, stepped, 0.0).astype(bf16)
            )
        mixed_ref[here, :] = out
        ending = running[length - 1 :, :]
        to_end = jnp.exp(wide_heads(ending - running, heads, lane))
        update = tn(write, (stepped * to_end).astype(bf16))
        state_s[...] = state_s[...] * reach[length - 1 :, :] + update
        return carry

    lax.fori_loop(0, planes, chunk, 0)
    state_ref[: SSM_STATE, :] = state_s[...].astype(bf16)
    total = wide_heads(base_s[...], heads, lane[:1])
    high = total.astype(bf16)
    rest = total - high.astype(f32)
    middle = rest.astype(bf16)
    least = (rest - middle.astype(f32)).astype(bf16)
    tail = jnp.concatenate(
        [high, middle, least, jnp.zeros((SSM_STATE // 8 - 3, channels), bf16)], axis=0
    )
    state_ref[SSM_STATE :, :] = tail


def finish_kernel(
    order_ref, states_ref, mixed_ref, reads_ref, gate_ref, run_ref, gain_ref, out_ref, into_s, *, heads
):
    count = states_ref.shape[0]
    here = order_ref[0]
    rows = mixed_ref.shape[0]
    channels = mixed_ref.shape[1]

    @pl.when(pl.program_id(0) == 0)
    def _():
        into_s[...] = jnp.zeros(into_s.shape, f32)

        def add(j, carry):
            piece = states_ref[here ^ j].astype(f32)
            decay = jnp.exp(
                piece[SSM_STATE : SSM_STATE + 1]
                + piece[SSM_STATE + 1 : SSM_STATE + 2]
                + piece[SSM_STATE + 2 : SSM_STATE + 3]
            )
            into_s[...] = into_s[...] * decay + piece[:SSM_STATE]
            return carry

        lax.fori_loop(0, here, add, 0)

    lane = lax.broadcasted_iota(jnp.int32, (rows, LANES), 1)
    reach = jnp.exp(wide_heads(run_ref[...], heads, lane))
    mixed = mixed_ref[...] + nn(reads_ref[...], into_s[...].astype(bf16)) * reach
    gated = mixed * jax.nn.silu(gate_ref[...].astype(f32))
    scale = lax.rsqrt(jnp.mean(gated * gated, axis=-1, keepdims=True) + eps)
    out_ref[...] = (gated * scale * gain_ref[...]).astype(bf16)


def params():
    return pltpu.CompilerParams(vmem_limit_bytes=60 * 1024 * 1024)


def shape(dims, kind):
    return jax.ShapeDtypeStruct(dims, kind)


def shards(
    tokens,
    mix_gain,
    query_proj,
    compressed_projection,
    compressed_norm_gain,
    rope_proj,
    key_up,
    value_up_weight,
    scan_input,
    scan_gate,
    scan_write,
    scan_read,
    step_proj,
    conv_input,
    conv_write,
    conv_read,
    decay_log,
    decay_offset,
    skip_gain,
    group_gain,
):
    A, B, T = lax.axis_size("a"), lax.axis_size("b"), lax.axis_size("tp")
    ia, ib, it = lax.axis_index("a"), lax.axis_index("b"), lax.axis_index("tp")
    ia, ib, it = ia.astype(jnp.int32), ib.astype(jnp.int32), it.astype(jnp.int32)
    sp_index = ia * B + ib
    rows, model = tokens.shape
    length = rows * T
    heads = key_up.shape[1] // UNROTATED_WIDTH
    latent_width = key_up.shape[0]
    groups = scan_write.shape[1] // SSM_STATE
    assert groups == B
    per_group = decay_log.shape[0] // groups
    channels = per_group * SSM_DIM
    depth = scan_write.shape[0]

    def by_group(values):
        return values.reshape(depth, groups, -1)

    packed = jnp.concatenate(
        [by_group(scan_input), by_group(scan_write), by_group(scan_read), by_group(scan_gate)],
        axis=2,
    )
    packed = jnp.transpose(packed, (1, 0, 2))
    if B > 1:
        packed = lax.all_to_all(packed, "b", 0, 0, tiled=True)
    columns = packed.shape[2]
    packed = packed.reshape(B * depth, columns)
    w_pieces = ring(packed, "a")

    own = pl.pallas_call(
        norm_kernel, out_shape=shape((rows, model), bf16), name="row_norm"
    )(tokens, mix_gain.reshape(1, -1))

    positions = sp_index * length + jnp.arange(length, dtype=jnp.int32)
    half = ROPE // 2
    freqs = theta ** (-jnp.arange(half, dtype=f32) * 2.0 / ROPE)
    angle = positions.astype(f32)[:, None] * jnp.tile(freqs, LANES // half)[None, :]
    sign = jnp.where(jnp.arange(LANES) % ROPE < half, -1.0, 1.0).astype(f32)
    cosine = jnp.cos(angle)
    sine = jnp.sin(angle) * sign[None, :]
    own_cos = lax.dynamic_slice_in_dim(cosine, it * rows, rows, 0)
    own_sin = lax.dynamic_slice_in_dim(sine, it * rows, rows, 0)

    key_own = pl.pallas_call(
        latent_kernel,
        out_shape=shape((rows, latent_width + 2 * ROPE), bf16),
        name="latent",
    )(
        own,
        compressed_projection,
        compressed_norm_gain.reshape(1, -1),
        rope_proj,
        own_cos,
        own_sin,
    )

    x_plane = exchange(own, "b")
    x_pieces = []
    x_places = []
    for k, piece in enumerate(x_plane):
        for t, part in enumerate(exchange(piece, "tp")):
            x_pieces.append(part)
            x_places.append((ib ^ k) * T + (it ^ t))
    x_order = jnp.stack(x_places)

    key_stack = jnp.stack(exchange(key_own, "a"))
    key_pieces = []
    key_places = []
    for k, piece in enumerate(exchange(key_stack, "b")):
        for t, part in enumerate(exchange(piece, "tp")):
            key_pieces.append(part)
            for z in range(A):
                key_places.append(((ia ^ z) * B + (ib ^ k)) * T + (it ^ t))
    key_order = jnp.stack(key_places + [sp_index])

    halo = lax.ppermute(own[rows - 8 :], "a", [(i, i + 1) for i in range(A - 1)])
    halo = jnp.where((ib == B - 1) & (it == T - 1), halo, jnp.zeros_like(halo))
    halo = spread_last(spread_last(halo, "b"), "tp")

    even = heads + heads % 2
    wq = query_proj
    if even != heads:
        wq = jnp.pad(wq, ((0, 0), (0, UNROTATED_WIDTH + ROPE)))
    q_order = jnp.stack([it ^ t for t in range(T)])
    plain, turned = pl.pallas_call(
        functools.partial(query_kernel, count=T, heads=even),
        in_specs=[smem()] + [vmem()] * (T + 3),
        out_shape=(
            shape((length, even * LANES), bf16),
            shape((length, even // 2 * LANES), bf16),
        ),
        compiler_params=params(),
        name="query",
    )(q_order, *x_pieces[:T], wq, cosine, sine)

    arrays = len(key_pieces)
    slots = A
    places = arrays * slots
    value_t = value_up_weight.T

    def attend(first, many):
        lo, hi = first * LANES, (first + many) * LANES
        pair = first // 2 * LANES
        return pl.pallas_call(
            functools.partial(
                attention_kernel, arrays=arrays, slots=slots, heads=many, blocks=A * B
            ),
            in_specs=[smem()] + [vmem()] * 4 + [hbm()] * arrays,
            out_specs=vmem(),
            out_shape=shape((length, many * VALUE_WIDTH), bf16),
            scratch_shapes=[
                pltpu.VMEM((places * rows, latent_width + 2 * ROPE), bf16),
                pltpu.VMEM((many, length, 2 * LANES), bf16),
                pltpu.VMEM((many, 1, length), f32),
                pltpu.VMEM((many, 1, length), f32),
                pltpu.VMEM((many, VALUE_WIDTH, length), f32),
                pltpu.SemaphoreType.DMA((places,)),
            ],
            compiler_params=params(),
            name="attention",
        )(
            key_order,
            plain[:, lo:hi],
            turned[:, pair : pair + (many + 1) // 2 * LANES],
            key_up[:, lo:hi],
            value_t[lo:hi],
            *key_pieces,
        )

    attended = attend(0, heads)

    local = decay_log.shape[0]
    step_w = lax.dynamic_slice_in_dim(step_proj, it * local + ib * per_group, per_group, 1)
    step_w = jnp.pad(step_w, ((0, 0), (0, LANES - per_group)))

    def mine(values, width):
        return lax.dynamic_slice_in_dim(values, ib * width, width, values.ndim - 1)

    taps = jnp.concatenate(
        [mine(conv_input, channels), mine(conv_write, SSM_STATE), mine(conv_read, SSM_STATE)],
        axis=1,
    ).astype(f32)
    rate = jnp.pad(-jnp.exp(mine(decay_log, per_group)), (0, LANES - per_group)).reshape(1, -1)
    skip = jnp.repeat(mine(skip_gain, per_group), SSM_DIM).reshape(1, -1)
    gain = mine(group_gain, channels).reshape(1, -1)
    offsets = decay_offset.T.reshape(groups, per_group, length)
    if B > 1:
        offsets = lax.all_to_all(offsets, "b", 0, 0, tiled=True)
    offsets = jnp.transpose(offsets, (0, 2, 1)).reshape(B * length, per_group)
    offsets = jnp.pad(offsets, ((0, 0), (0, LANES - per_group)))

    span = B * length
    w_order = jnp.stack([(ia - k) % A for k in range(A)]).astype(jnp.int32)
    conv = channels + 2 * SSM_STATE
    state_rows = SSM_STATE + SSM_STATE // 8
    mixed, reads, gate, run, state = pl.pallas_call(
        functools.partial(
            scan_kernel,
            planes=B,
            cores=T,
            weights=A,
            length=length,
            heads=per_group,
        ),
        in_specs=[smem(), smem()] + [hbm()] * (B * T + A) + [vmem()] * 6,
        out_specs=[vmem()] * 5,
        out_shape=(
            shape((span, channels), f32),
            shape((span, SSM_STATE), bf16),
            shape((span, channels), bf16),
            shape((span, LANES), f32),
            shape((state_rows, channels), bf16),
        ),
        scratch_shapes=[
            pltpu.VMEM((span, model), bf16),
            pltpu.VMEM((model, columns), bf16),
            pltpu.VMEM((8 + length, conv), f32),
            pltpu.VMEM((SSM_STATE, channels), f32),
            pltpu.VMEM((1, LANES), f32),
            pltpu.SemaphoreType.DMA((B * T,)),
            pltpu.SemaphoreType.DMA((A,)),
        ],
        compiler_params=params(),
        name="state_scan",
    )(x_order, w_order, *x_pieces, *w_pieces, halo, step_w, taps, rate, offsets, skip)

    states = jnp.stack(exchange(state, "a"))
    block = length
    scanned = pl.pallas_call(
        functools.partial(finish_kernel, heads=per_group),
        grid=(span // block,),
        in_specs=[
            smem(),
            pl.BlockSpec(states.shape, lambda i: (0, 0, 0)),
            pl.BlockSpec((block, channels), lambda i: (i, 0)),
            pl.BlockSpec((block, SSM_STATE), lambda i: (i, 0)),
            pl.BlockSpec((block, channels), lambda i: (i, 0)),
            pl.BlockSpec((block, LANES), lambda i: (i, 0)),
            pl.BlockSpec((1, channels), lambda i: (0, 0)),
        ],
        out_specs=pl.BlockSpec((block, channels), lambda i: (i, 0)),
        out_shape=shape((span, channels), bf16),
        scratch_shapes=[pltpu.VMEM((SSM_STATE, channels), f32)],
        compiler_params=params(),
        name="finish",
    )(ia.reshape(1), states, mixed, reads, gate, run, gain)
    if B > 1:
        scanned = scanned.reshape(B, length, channels)
        scanned = lax.all_to_all(scanned, "b", 0, 0, tiled=True)
        scanned = jnp.transpose(scanned, (1, 0, 2)).reshape(length, B * channels)
    return (attended, scanned)


def solution(mesh):
    S, T = mesh.shape["sp"], mesh.shape["tp"]
    sp = ("a", "b")
    in_specs = (
        P(("a", "b", "tp"), None),
        P(),
        P(None, "tp"),
        P(),
        P(),
        P(),
        P(None, "tp"),
        P(None, "tp"),
        P(sp, "tp"),
        P(sp, "tp"),
        P(sp, "tp"),
        P(sp, "tp"),
        P(),
        P(None, "tp"),
        P(None, "tp"),
        P(None, "tp"),
        P("tp"),
        P(sp, "tp"),
        P("tp"),
        P("tp"),
    )
    out_specs = (P(sp, "tp"), P(sp, "tp"))

    def run(*arrays):
        B = arrays[10].shape[1] // SSM_STATE // T
        assert S % B == 0
        fine = Mesh(mesh.devices.reshape(S // B, B, T), ("a", "b", "tp"))
        body = jax.shard_map(
            shards, mesh=fine, in_specs=in_specs, out_specs=out_specs, check_vma=False
        )
        return body(*arrays)

    return run
```

```python
import functools
import math

import jax
import jax.numpy as jnp
from jax import lax
from jax.experimental import pallas as pl
from jax.experimental.pallas import tpu as pltpu
from jax.sharding import Mesh
from jax.sharding import PartitionSpec as P


UNROTATED_WIDTH = 128
ROPE = 64
VALUE_WIDTH = 128
SSM_DIM = 64
SSM_STATE = 128

eps = 1e-06
theta = 10000.0
floor_score = -1e30
LANES = 128
DIRECT = 8


f32 = jnp.float32
bf16 = jnp.bfloat16


def vmem():
    return pl.BlockSpec(memory_space=pltpu.VMEM)


def smem():
    return pl.BlockSpec(memory_space=pltpu.SMEM)


def hbm():
    return pl.BlockSpec(memory_space=pl.ANY)


def nt(a, b):
    return lax.dot_general(a, b, (((1,), (1,)), ((), ())), preferred_element_type=f32)


def tn(a, b):
    return lax.dot_general(a, b, (((0,), (0,)), ((), ())), preferred_element_type=f32)


def nn(a, b, precision=None):
    return lax.dot_general(
        a, b, (((1,), (0,)), ((), ())), precision=precision, preferred_element_type=f32
    )


def exchange(value, axis):
    count = lax.axis_size(axis)
    if count == 1:
        return [value]
    assert count & (count - 1) == 0
    if count <= DIRECT:
        return [value] + [across(value, axis, k) for k in range(1, count)]
    everything = lax.all_gather(value, axis)
    here = lax.axis_index(axis)
    return [
        lax.dynamic_index_in_dim(everything, here ^ k, 0, keepdims=False) for k in range(count)
    ]


def across(value, axis, k):
    count = lax.axis_size(axis)
    return lax.ppermute(value, axis, [(i, i ^ k) for i in range(count)])


def ring(value, axis):
    count = lax.axis_size(axis)
    if count <= DIRECT:
        pieces = [value]
        for _ in range(1, count):
            pairs = [(i, (i + 1) % count) for i in range(count)]
            pieces.append(lax.ppermute(pieces[-1], axis, pairs))
        return pieces
    everything = lax.all_gather(value, axis)
    here = lax.axis_index(axis)
    return [
        lax.dynamic_index_in_dim(everything, (here - k) % count, 0, keepdims=False)
        for k in range(count)
    ]


def three_parts(values):
    high = lax.reduce_precision(values, 8, 7)
    rest = values - high
    middle = lax.reduce_precision(rest, 8, 7)
    return jnp.stack([high, middle, rest - middle]).astype(bf16)


def prologue_kernel(
    where_ref, tokens_ref, mix_ref, proj_ref, gain_ref, rope_ref, step_ref, cos_ref, sin_ref, rows_ref, key_ref
):
    tokens = tokens_ref[...].astype(f32)
    scale = lax.rsqrt(jnp.mean(tokens * tokens, axis=-1, keepdims=True) + eps)
    x = (tokens * scale * mix_ref[...]).astype(bf16)
    model = x.shape[1]
    rows_ref[:, :model] = x
    wide = nn(x, proj_ref[...])
    scale = lax.rsqrt(jnp.mean(wide * wide, axis=-1, keepdims=True) + eps)
    width = wide.shape[1]
    key_ref[:, :width] = (wide * scale * gain_ref[...]).astype(bf16)
    turn = nt(x, rope_ref[...])
    rope = turn.shape[1]
    half = rope // 2
    row = lax.broadcasted_iota(jnp.int32, (rope, 2 * rope), 0)
    col = lax.broadcasted_iota(jnp.int32, (rope, 2 * rope), 1) % rope
    same = (row == col).astype(f32)
    swap = (row == (col + half) % rope).astype(f32)
    best = lax.Precision.HIGHEST
    count = x.shape[0]
    here = pl.ds(pl.multiple_of(where_ref[2] * count, count), count)
    turned = nn(turn, same, best) * cos_ref[here, :] + nn(turn, swap, best) * sin_ref[here, :]
    key_ref[:, width:] = turned.astype(bf16)
    step = jax.nn.softplus(nt(x, step_ref[...]))
    count = step.shape[1]
    row = lax.broadcasted_iota(jnp.int32, (count, LANES), 0)
    col = lax.broadcasted_iota(jnp.int32, (count, LANES), 1)
    tail = jnp.zeros((x.shape[0], LANES), f32)
    for part in range(3):
        piece = step.astype(bf16)
        step = step - piece.astype(f32)
        tail = tail + nn(piece, (col == row + part * count).astype(f32).astype(bf16))
    rows_ref[:, model:] = tail.astype(bf16)


def query_kernel(where_ref, *refs, count, heads):
    pieces = refs[:count]
    w_ref, cos_ref, sin_ref, plain_ref, turned_ref = refs[count:]
    rows = pieces[0].shape[0]
    w = w_ref[...]
    lane = lax.broadcasted_iota(jnp.int32, (rows, LANES), 1)
    low = lane < ROPE
    first = lane % ROPE < ROPE // 2
    for k in range(count):
        start = pl.multiple_of((where_ref[2] ^ k) * rows, rows)
        here = pl.ds(start, rows)
        q = nn(pieces[k][:, : w.shape[0]], w).astype(bf16).astype(f32)
        cos = cos_ref[here, :]
        sin = sin_ref[here, :]
        for pair in range(heads // 2):
            base = pair * 3 * LANES
            t0 = q[:, base : base + LANES]
            t1 = q[:, base + LANES : base + 2 * LANES]
            t2 = q[:, base + 2 * LANES : base + 3 * LANES]
            odd = jnp.where(low, pltpu.roll(t1, ROPE, 1), pltpu.roll(t2, ROPE, 1))
            turn = jnp.where(low, t1, t2)
            other = jnp.where(
                first, pltpu.roll(turn, LANES - ROPE // 2, 1), pltpu.roll(turn, ROPE // 2, 1)
            )
            turned = turn * cos + other * sin
            at = pair * 2 * LANES
            plain_ref[here, at : at + LANES] = t0.astype(bf16)
            plain_ref[here, at + LANES : at + 2 * LANES] = odd.astype(bf16)
            turned_ref[here, pair * LANES : (pair + 1) * LANES] = turned.astype(bf16)


def attention_kernel(
    where_ref,
    plain_ref,
    turned_ref,
    ku_ref,
    vu_ref,
    *refs,
    planes,
    cores,
    slots,
    heads,
    lower,
    upper,
    final,
):
    arrays = planes * cores
    pieces = refs[:arrays]
    refs = refs[arrays:]
    if lower > 0:
        before, refs = refs[:3], refs[3:]
    if final:
        out_ref, top_s, sum_s, acc_s, keys, q_s, sems = refs
    else:
        top_s, sum_s, acc_s, keys, q_s, sems = refs
    length = plain_ref.shape[0]
    rows = length // cores
    width = ku_ref.shape[0]
    ia, ib, it = where_ref[0], where_ref[1], where_ref[2]
    here = ia * planes + ib
    last = jnp.minimum(here + 1, upper)
    factor = (UNROTATED_WIDTH + ROPE) ** -0.5 * math.log2(math.e)

    for k in range(planes):
        for t in range(cores):
            for z in range(slots):
                block = (ia ^ z) * planes + (ib ^ k)

                @pl.when((block >= lower) & (block < last))
                def _():
                    start = pl.multiple_of((block - lower) * length + (it ^ t) * rows, rows)
                    pltpu.make_async_copy(
                        pieces[k * cores + t].at[pl.ds(z * rows, rows), :],
                        keys.at[pl.ds(start, rows), :],
                        sems.at[block - lower],
                    ).start()

    lane = lax.broadcasted_iota(jnp.int32, (length, LANES), 1)
    for h in range(heads):
        q_s[h, :, :LANES] = plain_ref[:, h * LANES : (h + 1) * LANES]
        turned = turned_ref[:, (h // 2) * LANES : (h // 2 + 1) * LANES]
        keep = lane < ROPE if h % 2 == 0 else lane >= ROPE
        q_s[h, :, LANES:] = jnp.where(keep, turned, jnp.zeros_like(turned))
    if lower > 0:
        top_s[...] = before[0][...]
        sum_s[...] = before[1][...]
        acc_s[...] = before[2][...]
    else:
        top_s[...] = jnp.full(top_s.shape, floor_score, f32)
        sum_s[...] = jnp.zeros(sum_s.shape, f32)
        acc_s[...] = jnp.zeros(acc_s.shape, f32)

    def visit(block, masked):
        at = pl.ds(pl.multiple_of((block - lower) * length, length), length)
        pltpu.make_async_copy(keys.at[at, :], keys.at[at, :], sems.at[block - lower]).wait()
        latent = keys[at, :width]
        shared = keys[at, width:]
        key_plain = nn(latent, ku_ref[...]).astype(bf16)
        values = nt(vu_ref[...], latent).astype(bf16)
        if masked:
            key_at = lax.broadcasted_iota(jnp.int32, (length, length), 0)
            query_at = lax.broadcasted_iota(jnp.int32, (length, length), 1)
            seen = key_at <= query_at
        for h in range(heads):
            key = jnp.concatenate([key_plain[:, h * LANES : (h + 1) * LANES], shared], axis=1)
            score = nt(key, q_s[h])
            if masked:
                score = jnp.where(seen, score, -jnp.inf)
            old = top_s[h]
            top = jnp.maximum(old, jnp.max(score, axis=0, keepdims=True))
            weight = jnp.exp2((score - top) * factor)
            shrink = jnp.exp2((old - top) * factor)
            top_s[h] = top
            sum_s[h] = sum_s[h] * shrink + jnp.sum(weight, axis=0, keepdims=True)
            acc_s[h] = acc_s[h] * shrink + nn(
                values[h * VALUE_WIDTH : (h + 1) * VALUE_WIDTH, :], weight.astype(bf16)
            )

    def body(block, carry):
        visit(block, False)
        return carry

    lax.fori_loop(lower, jnp.minimum(here, upper), body, 0)

    @pl.when((here >= lower) & (here < upper))
    def _():
        visit(here, True)

    if final:
        for h in range(heads):
            result = (acc_s[h] / sum_s[h]).T
            out_ref[:, h * VALUE_WIDTH : (h + 1) * VALUE_WIDTH] = result.astype(bf16)


def wide_heads(values, heads, lane):
    tiles = []
    for pair in range(0, heads, 2):
        a = jnp.broadcast_to(values[:, pair : pair + 1], (values.shape[0], LANES))
        b = jnp.broadcast_to(values[:, pair + 1 : pair + 2], (values.shape[0], LANES))
        tiles.append(jnp.where(lane < SSM_DIM, a, b))
    return jnp.concatenate(tiles, axis=1)


def row_copies(where_ref, pieces, parts, target, sems, length, cores, width):
    ib, it = where_ref[1], where_ref[2]
    rows = length // cores
    for piece, (k, t, start, count) in zip(pieces, parts):
        block = ib ^ k
        at = pl.multiple_of(block * length + (it ^ t) * rows + start, count)
        yield pltpu.make_async_copy(
            piece.at[:, pl.ds(0, width)], target.at[pl.ds(at, count), :], sems.at[block]
        )


def weight_copies(where_ref, piece, plane, target, sem, planes):
    depth = piece.shape[0] // planes
    for k in range(planes):
        at = pl.multiple_of((plane * planes + (where_ref[1] ^ k)) * depth, depth)
        yield pltpu.make_async_copy(
            piece.at[pl.ds(k * depth, depth), :], target.at[pl.ds(at, depth), :], sem
        )


def scan_kernel(
    where_ref,
    *refs,
    parts,
    planes,
    cores,
    weights,
    length,
    heads,
    every,
):
    nx = len(parts)
    xs_in = refs[:nx]
    ws_in = refs[nx : nx + weights]
    halo_in = refs[nx + weights : nx + weights + planes * cores]
    (
        extra_ref,
        ci_ref,
        cw_ref,
        cr_ref,
        rate_ref,
        skip_ref,
        mixed_ref,
        reads_ref,
        run_ref,
        state_ref,
        xs,
        ws,
        hs,
        hx,
        pad,
        state_s,
        base_s,
        xsem,
        wsem,
        hsem,
    ) = refs[nx + weights + planes * cores :]
    ia, ib, it = where_ref[0], where_ref[1], where_ref[2]
    deep = ws_in[0].shape[0]
    channels = heads * SSM_DIM
    span = ci_ref.shape[0]
    tiles = hs.shape[0]
    bottom = halo_in[0].shape[0] - tiles
    for k in range(planes):
        for t in range(cores):

            @pl.when(((ib ^ k) == planes - 1) & ((it ^ t) == cores - 1))
            def _():
                pltpu.make_async_copy(
                    halo_in[k * cores + t].at[pl.ds(bottom, tiles), :], hs, hsem
                ).start()

    for k in range(weights):
        for copy in weight_copies(
            where_ref, ws_in[k], (ia - k + weights) % weights, ws, wsem.at[k], planes
        ):
            copy.start()
    for copy in row_copies(where_ref, xs_in, parts, xs, xsem, length, cores, xs.shape[1]):
        copy.start()
    state_s[...] = jnp.zeros(state_s.shape, f32)
    base_s[...] = jnp.zeros(base_s.shape, f32)
    pltpu.make_async_copy(hs, hs, hsem).wait()
    edge = hs[...].astype(f32)
    hx[...] = jnp.zeros(hx.shape, f32)
    for i in range(tiles):
        for r in range(span - 1):
            row = 8 - (span - 1) + r
            hx[row : row + 1, i * LANES : (i + 1) * LANES] = edge[
                i : i + 1, r * LANES : (r + 1) * LANES
            ]
    lane = lax.broadcasted_iota(jnp.int32, (length, LANES), 1)
    li = lax.broadcasted_iota(jnp.int32, (length, length), 0)
    si = lax.broadcasted_iota(jnp.int32, (length, length), 1)
    causal = si <= li
    tril = causal.astype(f32).astype(bf16)
    model = ws.shape[0]
    wide_lane = lax.broadcasted_iota(jnp.int32, (length, channels), 1)

    def onehot(rows, columns, test):
        source = lax.broadcasted_iota(jnp.int32, (rows, columns), 0)
        target = lax.broadcasted_iota(jnp.int32, (rows, columns), 1)
        return test(source, target).astype(f32)

    local = rate_ref.shape[1]
    best = lax.Precision.HIGHEST
    first = it * local + ib * heads
    pick = onehot(
        LANES,
        LANES,
        lambda i, j: (i % every == first + j % heads) & (i < 3 * every) & (j < 3 * heads),
    ).astype(bf16)
    pick_offset = onehot(
        16, LANES, lambda i, j: (i % heads == j % heads) & (i < 3 * heads) & (j < 3 * heads)
    ).astype(bf16)
    pick_rate = onehot(local, LANES, lambda i, j: (i == ib * heads + j % heads) & (j < 3 * heads))
    pick_skip = onehot(local, channels, lambda i, j: i == ib * heads + j // SSM_DIM)
    rate = -jnp.exp(jnp.broadcast_to(rate_ref[...], (8, local)))
    rate = nn(rate, pick_rate, best)[:1]
    skip = nn(jnp.broadcast_to(skip_ref[...], (8, local)), pick_skip, best)[:1]

    def mine(ref, width):
        return ref[:, pl.ds(pl.multiple_of(ib * width, width), width)].astype(f32)

    taps = jnp.concatenate(
        [mine(ci_ref, channels), mine(cw_ref, SSM_STATE), mine(cr_ref, SSM_STATE)], axis=1
    )
    for k in range(weights):
        pltpu.make_async_copy(ws_in[k], ws.at[pl.ds(0, deep), :], wsem.at[k]).wait()
    pad[0:8, :] = nn(hx[...].astype(bf16), ws[...]).astype(bf16).astype(f32)

    def chunk(c, carry):
        here = pl.ds(pl.multiple_of(c * length, length), length)
        pltpu.make_async_copy(xs.at[here, :], xs.at[here, :], xsem.at[c]).wait()
        raw = nn(xs[here, :model], ws[...]).astype(bf16)
        pad[8:, :] = raw.astype(f32)
        total = jnp.zeros(raw.shape, f32)
        for k in range(span):
            total = total + taps[k : k + 1, :] * pad[8 - span + 1 + k : 8 - span + 1 + k + length, :]
        mixed_in = jax.nn.silu(total).astype(bf16)
        pad[0:8, :] = pad[length : length + 8, :]
        head = mixed_in[:, :channels].astype(f32)
        write = mixed_in[:, channels : channels + SSM_STATE]
        read = mixed_in[:, channels + SSM_STATE :]
        reads_ref[here, :] = read
        step = nn(xs[here, model:], pick)
        offset = tn(extra_ref[ib ^ c], pick_offset)
        decay = rate * step + offset
        high = decay.astype(bf16)
        rest = decay - high.astype(f32)
        middle = rest.astype(bf16)
        least = rest - middle.astype(f32)
        split = jnp.where(lane < heads, high.astype(f32), middle.astype(f32))
        split = jnp.where(lane < 2 * heads, split, least).astype(bf16)
        running = nn(tril, split)
        running = (
            running
            + pltpu.roll(running, LANES - heads, 1)
            + pltpu.roll(running, LANES - 2 * heads, 1)
        )
        run_ref[here, :] = running + base_s[...]
        base_s[...] = base_s[...] + running[length - 1 :, :]
        across = running.T
        stepped = head * wide_heads(step, heads, lane)
        inner = nt(read, write)
        reach = jnp.exp(wide_heads(running, heads, lane))
        out = nn(read, state_s[...].astype(bf16)) * reach + skip * head
        for h in range(heads):
            spread = running[:, h : h + 1] - across[h : h + 1, :]
            fading = jnp.exp(jnp.where(causal, spread, floor_score))
            mine = (wide_lane >= h * SSM_DIM) & (wide_lane < (h + 1) * SSM_DIM)
            out = out + nn(
                (inner * fading).astype(bf16), jnp.where(mine, stepped, 0.0).astype(bf16)
            )
        mixed_ref[here, :] = out
        ending = running[length - 1 :, :]
        to_end = jnp.exp(wide_heads(ending - running, heads, lane))
        update = tn(write, (stepped * to_end).astype(bf16))
        state_s[...] = state_s[...] * reach[length - 1 :, :] + update
        return carry

    lax.fori_loop(0, planes, chunk, 0)
    state_ref[: SSM_STATE, :] = state_s[...].astype(bf16)
    total = wide_heads(base_s[...], heads, lane[:1])
    high = total.astype(bf16)
    rest = total - high.astype(f32)
    middle = rest.astype(bf16)
    least = (rest - middle.astype(f32)).astype(bf16)
    tail = jnp.concatenate(
        [high, middle, least, jnp.zeros((SSM_STATE // 8 - 3, channels), bf16)], axis=0
    )
    state_ref[SSM_STATE :, :] = tail


def gate_kernel(where_ref, *refs, parts, planes, cores, weights, length):
    nx = len(parts)
    xs_in = refs[:nx]
    ws_in = refs[nx : nx + weights]
    out_ref, xs, ws, xsem, wsem = refs[nx + weights :]
    ia = where_ref[0]
    deep = ws_in[0].shape[0]
    model = ws.shape[0]

    for k in range(weights):
        for copy in weight_copies(where_ref, ws_in[k], ia ^ k, ws, wsem.at[k], planes):
            copy.start()
    for copy in row_copies(where_ref, xs_in, parts, xs, xsem, length, cores, model):
        copy.start()
    for k in range(weights):
        pltpu.make_async_copy(ws_in[k], ws.at[pl.ds(0, deep), :], wsem.at[k]).wait()
    batch = 2 if planes % 2 == 0 else 1

    def some(c, carry):
        for i in range(batch):
            block = c * batch + i
            at = pl.ds(pl.multiple_of(block * length, length), length)
            pltpu.make_async_copy(xs.at[at, :], xs.at[at, :], xsem.at[block]).wait()
        here = pl.ds(pl.multiple_of(c * batch * length, batch * length), batch * length)
        out_ref[here, :] = jax.nn.silu(nn(xs[here, :], ws[...]).astype(bf16).astype(f32))
        return carry

    lax.fori_loop(0, planes // batch, some, 0)


def finish_kernel(
    where_ref, states_ref, mixed_ref, reads_ref, gate_ref, run_ref, gain_ref, out_ref, into_s, *, heads
):
    here = where_ref[0]
    rows = mixed_ref.shape[0]
    channels = mixed_ref.shape[1]

    @pl.when(pl.program_id(0) == 0)
    def _():
        into_s[...] = jnp.zeros(into_s.shape, f32)

        def add(j, carry):
            piece = states_ref[here ^ j].astype(f32)
            decay = jnp.exp(
                piece[SSM_STATE : SSM_STATE + 1]
                + piece[SSM_STATE + 1 : SSM_STATE + 2]
                + piece[SSM_STATE + 2 : SSM_STATE + 3]
            )
            into_s[...] = into_s[...] * decay + piece[:SSM_STATE]
            return carry

        lax.fori_loop(0, here, add, 0)

    lane = lax.broadcasted_iota(jnp.int32, (rows, LANES), 1)
    reach = jnp.exp(wide_heads(run_ref[...], heads, lane))
    mixed = mixed_ref[...] + nn(reads_ref[...], into_s[...].astype(bf16)) * reach
    gated = mixed * gate_ref[...]
    scale = lax.rsqrt(jnp.mean(gated * gated, axis=-1, keepdims=True) + eps)
    gain = gain_ref[:, pl.ds(pl.multiple_of(where_ref[1] * channels, channels), channels)]
    out_ref[...] = (gated * scale * gain).astype(bf16)


def params():
    return pltpu.CompilerParams(vmem_limit_bytes=60 * 1024 * 1024)


def cost(flops):
    return pl.CostEstimate(flops=flops, bytes_accessed=flops // 1000, transcendentals=0)


def shape(dims, kind):
    return jax.ShapeDtypeStruct(dims, kind)


def shards(
    tokens,
    mix_gain,
    query_proj,
    compressed_projection,
    compressed_norm_gain,
    rope_proj,
    key_up,
    value_up_weight,
    scan_input,
    scan_gate,
    scan_write,
    scan_read,
    step_proj,
    conv_input,
    conv_write,
    conv_read,
    decay_log,
    decay_offset,
    skip_gain,
    group_gain,
):
    A, B, T = lax.axis_size("a"), lax.axis_size("b"), lax.axis_size("tp")
    ia, ib, it = (lax.axis_index(name).astype(jnp.int32) for name in ("a", "b", "tp"))
    where = jnp.stack([ia, ib, it])
    rows, model = tokens.shape
    length = rows * T
    heads = key_up.shape[1] // UNROTATED_WIDTH
    key_width = key_up.shape[0] + 2 * ROPE
    groups = scan_write.shape[1] // SSM_STATE
    local = decay_log.shape[0]
    per_group = local // groups
    channels = per_group * SSM_DIM
    depth = scan_write.shape[0]
    every = step_proj.shape[1]
    taps = conv_input.shape[0]
    span = B * length
    assert groups == B and channels == length
    assert 3 * every <= LANES and 3 * per_group <= 16
    assert (taps - 1) * LANES == key_width

    def regrouped(pieces):
        moved = []
        for k in range(B):
            group = ib ^ k
            parts = [
                lax.dynamic_slice_in_dim(piece, group * width, width, 1)
                for piece, width in pieces
            ]
            value = parts[0] if len(parts) == 1 else jnp.concatenate(parts, axis=1)
            moved.append(across(value, "b", k) if k else value)
        return moved

    positions = (ia * B + ib) * length + jnp.arange(length, dtype=jnp.int32)
    half = ROPE // 2
    freqs = theta ** (-jnp.arange(half, dtype=f32) * 2.0 / ROPE)
    angle = positions.astype(f32)[:, None] * jnp.tile(freqs, LANES // half)[None, :]
    sign = jnp.where(jnp.arange(LANES) % ROPE < half, -1.0, 1.0).astype(f32)
    cosine = jnp.cos(angle)
    sine = jnp.sin(angle) * sign[None, :]

    own, key_own = pl.pallas_call(
        prologue_kernel,
        in_specs=[smem()] + [vmem()] * 8,
        out_shape=(shape((rows, model + LANES), bf16), shape((rows, key_width), bf16)),
        compiler_params=params(),
        cost_estimate=cost(2 * rows * model * 1024),
        name="prologue",
    )(
        where,
        tokens,
        mix_gain.reshape(1, -1),
        compressed_projection,
        compressed_norm_gain.reshape(1, -1),
        rope_proj.T,
        step_proj.T,
        cosine,
        sine,
    )
    scan_input, key_own = lax.optimization_barrier((scan_input, key_own))
    packed = regrouped([(scan_input, channels), (scan_write, SSM_STATE), (scan_read, SSM_STATE)])
    packed = jnp.concatenate(packed, axis=0)

    edge = lax.ppermute(
        own[rows - taps + 1 :, :model], "a", [(i, i + 1) for i in range(A - 1)]
    )
    edge = edge.reshape(taps - 1, model // LANES, LANES)
    edge = jnp.transpose(edge, (1, 0, 2)).reshape(model // LANES, key_width)
    key_stack = jnp.concatenate(exchange(key_own, "a") + [edge], axis=0)
    packed, key_stack = lax.optimization_barrier((packed, key_stack))
    w_pieces = ring(packed, "a")
    key_pieces = []
    for piece in exchange(key_stack, "b"):
        key_pieces += exchange(piece, "tp")

    if B == 4:
        side, front = across(own, "b", 1), across(own, "b", 2)
        some = rows // 2
        far = [across(side[:some], "b", 2), across(front[some:], "b", 1)]
        plane = [(0, 0, own), (1, 0, side), (2, 0, front), (3, 0, far[0]), (3, some, far[1])]
    else:
        plane = [(k, 0, piece) for k, piece in enumerate(exchange(own, "b"))]
    x_pieces = []
    parts = []
    for k, start, piece in plane:
        for t, part in enumerate(exchange(piece, "tp")):
            x_pieces.append(part)
            parts.append((k, t, start, part.shape[0]))

    offsets = three_parts(decay_offset.T).reshape(3, groups, per_group, length)
    offsets = jnp.transpose(offsets, (1, 0, 2, 3)).reshape(groups, 3 * per_group, length)
    offsets = jnp.pad(offsets, ((0, 0), (0, 16 - 3 * per_group), (0, 0)))
    offsets = jnp.transpose(offsets, (1, 0, 2)).reshape(16, groups * length)
    extra = regrouped([(jnp.concatenate([scan_gate, offsets], axis=0), channels)])
    g_pieces = exchange(jnp.concatenate([e[:depth] for e in extra], axis=0), "a")
    tails = jnp.stack([e[depth:] for e in extra])
    value_t = value_up_weight.T

    even = heads + heads % 2
    wq = query_proj
    if even != heads:
        wq = jnp.pad(wq, ((0, 0), (0, UNROTATED_WIDTH + ROPE)))
    plain, turned = pl.pallas_call(
        functools.partial(query_kernel, count=T, heads=even),
        in_specs=[smem()] + [vmem()] * (T + 3),
        out_shape=(shape((length, even * LANES), bf16), shape((length, even // 2 * LANES), bf16)),
        compiler_params=params(),
        cost_estimate=cost(2 * length * model * even * 256),
        name="query",
    )(where, *x_pieces[:T], wq, cosine, sine)

    def attend(place, lower, upper, carry):
        final = upper == A * B
        carried = (
            shape((heads, 1, length), f32),
            shape((heads, 1, length), f32),
            shape((heads, VALUE_WIDTH, length), f32),
        )
        outs = (shape((length, heads * VALUE_WIDTH), bf16),) if final else carried
        scratch = [pltpu.VMEM(c.shape, f32) for c in carried] if final else []
        return pl.pallas_call(
            functools.partial(
                attention_kernel,
                planes=B,
                cores=T,
                slots=A,
                heads=heads,
                lower=lower,
                upper=upper,
                final=final,
            ),
            in_specs=[smem()] + [vmem()] * 4 + [hbm()] * (B * T) + [vmem()] * len(carry),
            out_specs=tuple(vmem() for _ in outs),
            out_shape=outs,
            scratch_shapes=scratch
            + [
                pltpu.VMEM(((upper - lower) * length, key_width), bf16),
                pltpu.VMEM((heads, length, 2 * LANES), bf16),
                pltpu.SemaphoreType.DMA((upper - lower,)),
            ],
            compiler_params=params(),
            cost_estimate=cost(4 * length * (upper - lower) * length * LANES * 8),
            name="attention",
        )(place, plain, turned, key_up, value_t, *key_pieces, *carry)

    first_part = (3 * A * B) // 4
    carry = attend(where, 0, first_part, ())
    then, carry = lax.optimization_barrier((where, carry))

    conv = channels + 2 * SSM_STATE
    mixed, reads, run, state = pl.pallas_call(
        functools.partial(
            scan_kernel,
            parts=tuple(parts),
            planes=B,
            cores=T,
            weights=A,
            length=length,
            heads=per_group,
            every=every,
        ),
        in_specs=[smem()] + [hbm()] * (len(parts) + A + B * T) + [vmem()] * 6,
        out_specs=[vmem()] * 4,
        out_shape=(
            shape((span, channels), f32),
            shape((span, SSM_STATE), bf16),
            shape((span, LANES), f32),
            shape((SSM_STATE + SSM_STATE // 8, channels), bf16),
        ),
        scratch_shapes=[
            pltpu.VMEM((span, model + LANES), bf16),
            pltpu.VMEM((model, conv), bf16),
            pltpu.VMEM((model // LANES, key_width), bf16),
            pltpu.VMEM((8, model), f32),
            pltpu.VMEM((8 + length, conv), f32),
            pltpu.VMEM((SSM_STATE, channels), f32),
            pltpu.VMEM((1, LANES), f32),
            pltpu.SemaphoreType.DMA((B,)),
            pltpu.SemaphoreType.DMA((A,)),
            pltpu.SemaphoreType.DMA,
        ],
        compiler_params=params(),
        cost_estimate=cost(4 * span * model * conv),
        name="state_scan",
    )(
        then,
        *x_pieces,
        *w_pieces,
        *key_pieces,
        tails,
        conv_input,
        conv_write,
        conv_read,
        decay_log.reshape(1, -1),
        skip_gain.reshape(1, -1),
    )

    states = jnp.stack(exchange(state, "a"))
    then, mixed = lax.optimization_barrier((then, mixed))
    gate = pl.pallas_call(
        functools.partial(
            gate_kernel, parts=tuple(parts), planes=B, cores=T, weights=A, length=length
        ),
        in_specs=[smem()] + [hbm()] * (len(parts) + A),
        out_specs=vmem(),
        out_shape=shape((span, channels), f32),
        scratch_shapes=[
            pltpu.VMEM((span, model), bf16),
            pltpu.VMEM((model, channels), bf16),
            pltpu.SemaphoreType.DMA((B,)),
            pltpu.SemaphoreType.DMA((A,)),
        ],
        compiler_params=params(),
        cost_estimate=cost(2 * span * model * channels),
        name="gate",
    )(then, *x_pieces, *g_pieces)

    scanned = pl.pallas_call(
        functools.partial(finish_kernel, heads=per_group),
        grid=(B,),
        in_specs=[
            smem(),
            pl.BlockSpec(states.shape, lambda i: (0, 0, 0)),
            pl.BlockSpec((length, channels), lambda i: (i, 0)),
            pl.BlockSpec((length, SSM_STATE), lambda i: (i, 0)),
            pl.BlockSpec((length, channels), lambda i: (i, 0)),
            pl.BlockSpec((length, LANES), lambda i: (i, 0)),
            pl.BlockSpec((1, group_gain.shape[0]), lambda i: (0, 0)),
        ],
        out_specs=pl.BlockSpec((length, channels), lambda i: (i, 0)),
        out_shape=shape((span, channels), bf16),
        scratch_shapes=[pltpu.VMEM((SSM_STATE, channels), f32)],
        compiler_params=params(),
        name="finish",
    )(where, states, mixed, reads, gate, run, group_gain.reshape(1, -1))
    last, scanned = lax.optimization_barrier((then, scanned))
    (attended,) = attend(last, first_part, A * B, carry)
    if B > 1:
        scanned = lax.all_to_all(scanned.reshape(B, length, channels), "b", 0, 0, tiled=True)
        scanned = jnp.transpose(scanned, (1, 0, 2)).reshape(length, B * channels)
    return (attended, scanned)


def solution(mesh):
    S, T = mesh.shape["sp"], mesh.shape["tp"]
    sp = ("a", "b")
    in_specs = (
        P(("a", "b", "tp"), None),
        P(),
        P(None, "tp"),
        P(),
        P(),
        P(),
        P(None, "tp"),
        P(None, "tp"),
        P(sp, "tp"),
        P(sp, "tp"),
        P(sp, "tp"),
        P(sp, "tp"),
        P(),
        P(None, "tp"),
        P(None, "tp"),
        P(None, "tp"),
        P("tp"),
        P(sp, "tp"),
        P("tp"),
        P("tp"),
    )
    out_specs = (P(sp, "tp"), P(sp, "tp"))

    def run(*arrays):
        B = arrays[10].shape[1] // SSM_STATE // T
        assert S % B == 0
        fine = Mesh(mesh.devices.reshape(S // B, B, T), ("a", "b", "tp"))
        body = jax.shard_map(
            shards, mesh=fine, in_specs=in_specs, out_specs=out_specs, check_vma=False
        )
        return body(*arrays)

    return run
```

```python
import functools
import math

import jax
import jax.numpy as jnp
from jax import lax
from jax.experimental import pallas as pl
from jax.experimental.pallas import tpu as pltpu
from jax.sharding import Mesh
from jax.sharding import PartitionSpec as P


UNROTATED_WIDTH = 128
ROPE = 64
VALUE_WIDTH = 128
SSM_DIM = 64
SSM_STATE = 128

eps = 1e-06
theta = 10000.0
floor_score = -1e30
LANES = 128
DIRECT = 8


f32 = jnp.float32
bf16 = jnp.bfloat16


def vmem():
    return pl.BlockSpec(memory_space=pltpu.VMEM)


def smem():
    return pl.BlockSpec(memory_space=pltpu.SMEM)


def hbm():
    return pl.BlockSpec(memory_space=pl.ANY)


def nt(a, b):
    return lax.dot_general(a, b, (((1,), (1,)), ((), ())), preferred_element_type=f32)


def tn(a, b):
    return lax.dot_general(a, b, (((0,), (0,)), ((), ())), preferred_element_type=f32)


def nn(a, b, precision=None):
    return lax.dot_general(
        a, b, (((1,), (0,)), ((), ())), precision=precision, preferred_element_type=f32
    )


def exchange(value, axis):
    count = lax.axis_size(axis)
    if count == 1:
        return [value]
    assert count & (count - 1) == 0
    if count <= DIRECT:
        return [value] + [across(value, axis, k) for k in range(1, count)]
    everything = lax.all_gather(value, axis)
    here = lax.axis_index(axis)
    return [
        lax.dynamic_index_in_dim(everything, here ^ k, 0, keepdims=False) for k in range(count)
    ]


def across(value, axis, k):
    count = lax.axis_size(axis)
    return lax.ppermute(value, axis, [(i, i ^ k) for i in range(count)])


def ring(value, axis):
    count = lax.axis_size(axis)
    if count <= DIRECT:
        pieces = [value] + [None] * (count - 1)
        for way, steps in ((1, count // 2), (-1, (count - 1) // 2)):
            moving = value
            for step in range(1, steps + 1):
                place = way * step % count
                pairs = [(i, (i + way) % count) for i in range(count)]
                moving = lax.ppermute(moving, axis, pairs)
                pieces[place] = moving
        return pieces
    everything = lax.all_gather(value, axis)
    here = lax.axis_index(axis)
    return [
        lax.dynamic_index_in_dim(everything, (here - k) % count, 0, keepdims=False)
        for k in range(count)
    ]


def three_parts(values):
    high = lax.reduce_precision(values, 8, 7)
    rest = values - high
    middle = lax.reduce_precision(rest, 8, 7)
    return jnp.stack([high, middle, rest - middle]).astype(bf16)


def prologue_kernel(
    where_ref, tokens_ref, mix_ref, proj_ref, gain_ref, rope_ref, step_ref, cos_ref, sin_ref, rows_ref, key_ref, edge_ref
):
    tokens = tokens_ref[...].astype(f32)
    scale = lax.rsqrt(jnp.mean(tokens * tokens, axis=-1, keepdims=True) + eps)
    x = (tokens * scale * mix_ref[...]).astype(bf16)
    model = x.shape[1]
    rows_ref[:, :model] = x
    edge_ref[...] = x[x.shape[0] - edge_ref.shape[0] :, :]
    wide = nn(x, proj_ref[...])
    scale = lax.rsqrt(jnp.mean(wide * wide, axis=-1, keepdims=True) + eps)
    width = wide.shape[1]
    key_ref[:, :width] = (wide * scale * gain_ref[...]).astype(bf16)
    turn = nt(x, rope_ref[...])
    rope = turn.shape[1]
    half = rope // 2
    row = lax.broadcasted_iota(jnp.int32, (rope, 2 * rope), 0)
    col = lax.broadcasted_iota(jnp.int32, (rope, 2 * rope), 1) % rope
    same = (row == col).astype(f32)
    swap = (row == (col + half) % rope).astype(f32)
    best = lax.Precision.HIGHEST
    count = x.shape[0]
    here = pl.ds(pl.multiple_of(where_ref[2] * count, count), count)
    turned = nn(turn, same, best) * cos_ref[here, :] + nn(turn, swap, best) * sin_ref[here, :]
    key_ref[:, width:] = turned.astype(bf16)
    step = jax.nn.softplus(nt(x, step_ref[...]))
    count = step.shape[1]
    row = lax.broadcasted_iota(jnp.int32, (count, LANES), 0)
    col = lax.broadcasted_iota(jnp.int32, (count, LANES), 1)
    tail = jnp.zeros((x.shape[0], LANES), f32)
    for part in range(3):
        piece = step.astype(bf16)
        step = step - piece.astype(f32)
        tail = tail + nn(piece, (col == row + part * count).astype(f32).astype(bf16))
    rows_ref[:, model:] = tail.astype(bf16)


def query_kernel(where_ref, *refs, count, heads):
    pieces = refs[:count]
    w_ref, cos_ref, sin_ref, plain_ref, turned_ref = refs[count:]
    rows = pieces[0].shape[0]
    w = w_ref[...]
    lane = lax.broadcasted_iota(jnp.int32, (rows, LANES), 1)
    low = lane < ROPE
    first = lane % ROPE < ROPE // 2
    for k in range(count):
        start = pl.multiple_of((where_ref[2] ^ k) * rows, rows)
        here = pl.ds(start, rows)
        q = nn(pieces[k][:, : w.shape[0]], w).astype(bf16).astype(f32)
        cos = cos_ref[here, :]
        sin = sin_ref[here, :]
        for pair in range(heads // 2):
            base = pair * 3 * LANES
            t0 = q[:, base : base + LANES]
            t1 = q[:, base + LANES : base + 2 * LANES]
            t2 = q[:, base + 2 * LANES : base + 3 * LANES]
            odd = jnp.where(low, pltpu.roll(t1, ROPE, 1), pltpu.roll(t2, ROPE, 1))
            turn = jnp.where(low, t1, t2)
            other = jnp.where(
                first, pltpu.roll(turn, LANES - ROPE // 2, 1), pltpu.roll(turn, ROPE // 2, 1)
            )
            turned = turn * cos + other * sin
            at = pair * 2 * LANES
            plain_ref[here, at : at + LANES] = t0.astype(bf16)
            plain_ref[here, at + LANES : at + 2 * LANES] = odd.astype(bf16)
            turned_ref[here, pair * LANES : (pair + 1) * LANES] = turned.astype(bf16)


def attention_kernel(
    where_ref,
    plain_ref,
    turned_ref,
    ku_ref,
    vu_ref,
    *refs,
    planes,
    cores,
    slots,
    heads,
    lower,
    upper,
    final,
):
    arrays = planes * cores
    pieces = refs[:arrays]
    refs = refs[arrays:]
    if lower > 0:
        before, refs = refs[:3], refs[3:]
    if final:
        out_ref, top_s, sum_s, acc_s, keys, q_s, sems = refs
    else:
        top_s, sum_s, acc_s, keys, q_s, sems = refs
    length = plain_ref.shape[0]
    rows = length // cores
    width = ku_ref.shape[0]
    ia, ib, it = where_ref[0], where_ref[1], where_ref[2]
    here = ia * planes + ib
    last = jnp.minimum(here + 1, upper)
    factor = (UNROTATED_WIDTH + ROPE) ** -0.5 * math.log2(math.e)

    for k in range(planes):
        for t in range(cores):
            for z in range(slots):
                block = (ia ^ z) * planes + (ib ^ k)

                @pl.when((block >= lower) & (block < last))
                def _():
                    start = pl.multiple_of((block - lower) * length + (it ^ t) * rows, rows)
                    pltpu.make_async_copy(
                        pieces[k * cores + t].at[pl.ds(z * rows, rows), :],
                        keys.at[pl.ds(start, rows), :],
                        sems.at[block - lower],
                    ).start()

    lane = lax.broadcasted_iota(jnp.int32, (length, LANES), 1)
    for h in range(heads):
        q_s[h, :, :LANES] = plain_ref[:, h * LANES : (h + 1) * LANES]
        turned = turned_ref[:, (h // 2) * LANES : (h // 2 + 1) * LANES]
        keep = lane < ROPE if h % 2 == 0 else lane >= ROPE
        q_s[h, :, LANES:] = jnp.where(keep, turned, jnp.zeros_like(turned))
    if lower > 0:
        top_s[...] = before[0][...]
        sum_s[...] = before[1][...]
        acc_s[...] = before[2][...]
    else:
        top_s[...] = jnp.full(top_s.shape, floor_score, f32)
        sum_s[...] = jnp.zeros(sum_s.shape, f32)
        acc_s[...] = jnp.zeros(acc_s.shape, f32)

    def visit(block, masked):
        at = pl.ds(pl.multiple_of((block - lower) * length, length), length)
        pltpu.make_async_copy(keys.at[at, :], keys.at[at, :], sems.at[block - lower]).wait()
        latent = keys[at, :width]
        shared = keys[at, width:]
        key_plain = nn(latent, ku_ref[...]).astype(bf16)
        values = nt(vu_ref[...], latent).astype(bf16)
        if masked:
            key_at = lax.broadcasted_iota(jnp.int32, (length, length), 0)
            query_at = lax.broadcasted_iota(jnp.int32, (length, length), 1)
            seen = key_at <= query_at
        for h in range(heads):
            key = jnp.concatenate([key_plain[:, h * LANES : (h + 1) * LANES], shared], axis=1)
            score = nt(key, q_s[h])
            if masked:
                score = jnp.where(seen, score, -jnp.inf)
            old = top_s[h]
            top = jnp.maximum(old, jnp.max(score, axis=0, keepdims=True))
            weight = jnp.exp2((score - top) * factor)
            shrink = jnp.exp2((old - top) * factor)
            top_s[h] = top
            sum_s[h] = sum_s[h] * shrink + jnp.sum(weight, axis=0, keepdims=True)
            acc_s[h] = acc_s[h] * shrink + nn(
                values[h * VALUE_WIDTH : (h + 1) * VALUE_WIDTH, :], weight.astype(bf16)
            )

    def body(block, carry):
        visit(block, False)
        return carry

    lax.fori_loop(lower, jnp.minimum(here, upper), body, 0)

    @pl.when((here >= lower) & (here < upper))
    def _():
        visit(here, True)

    if final:
        for h in range(heads):
            result = (acc_s[h] / sum_s[h]).T
            out_ref[:, h * VALUE_WIDTH : (h + 1) * VALUE_WIDTH] = result.astype(bf16)


def wide_heads(values, heads, lane):
    tiles = []
    for pair in range(0, heads, 2):
        a = jnp.broadcast_to(values[:, pair : pair + 1], (values.shape[0], LANES))
        b = jnp.broadcast_to(values[:, pair + 1 : pair + 2], (values.shape[0], LANES))
        tiles.append(jnp.where(lane < SSM_DIM, a, b))
    return jnp.concatenate(tiles, axis=1)


def row_copies(where_ref, pieces, parts, target, sems, length, cores, width):
    ib, it = where_ref[1], where_ref[2]
    rows = length // cores
    for piece, (k, t, start, count) in zip(pieces, parts):
        block = ib ^ k
        at = pl.multiple_of(block * length + (it ^ t) * rows + start, count)
        yield pltpu.make_async_copy(
            piece.at[:, pl.ds(0, width)], target.at[pl.ds(at, count), :], sems.at[block]
        )


def weight_copies(where_ref, piece, plane, target, sem, planes):
    depth = piece.shape[0] // planes
    for k in range(planes):
        at = pl.multiple_of((plane * planes + (where_ref[1] ^ k)) * depth, depth)
        yield pltpu.make_async_copy(
            piece.at[pl.ds(k * depth, depth), :], target.at[pl.ds(at, depth), :], sem
        )


def scan_kernel(
    where_ref,
    *refs,
    parts,
    planes,
    cores,
    weights,
    length,
    heads,
    every,
):
    nx = len(parts)
    xs_in = refs[:nx]
    ws_in = refs[nx : nx + weights]
    tails_in = refs[nx + weights : nx + weights + planes * cores]
    (
        ci_ref,
        cw_ref,
        cr_ref,
        rate_ref,
        skip_ref,
        mixed_ref,
        reads_ref,
        gate_ref,
        run_ref,
        state_ref,
        xs,
        ws,
        hx,
        raws,
        state_s,
        base_s,
        xsem,
        wsem,
        tails,
        tsem,
    ) = refs[nx + weights + planes * cores :]
    ia, ib, it = where_ref[0], where_ref[1], where_ref[2]
    deep = ws_in[0].shape[0]
    channels = heads * SSM_DIM
    conv = channels + 2 * SSM_STATE
    span = ci_ref.shape[0]
    bottom = tails_in[0].shape[0] - tails.shape[1]
    for k in range(planes):
        for t in range(cores):
            piece = tails_in[k * cores + t].at[pl.ds(bottom, tails.shape[1]), :]
            if t == 0:
                pltpu.make_async_copy(piece, tails.at[k], tsem.at[k]).start()

            @pl.when(((ib ^ k) == planes - 1) & ((it ^ t) == cores - 1))
            def _():
                pltpu.make_async_copy(piece, tails.at[planes], tsem.at[planes]).start()

    for k in range(weights):
        for copy in weight_copies(
            where_ref, ws_in[k], (ia - k + weights) % weights, ws, wsem.at[k], planes
        ):
            copy.start()
    for copy in row_copies(where_ref, xs_in, parts, xs, xsem, length, cores, xs.shape[1]):
        copy.start()
    state_s[...] = jnp.zeros(state_s.shape, f32)
    base_s[...] = jnp.zeros(base_s.shape, f32)
    for k in range(planes):
        pltpu.make_async_copy(tails.at[k], tails.at[k], tsem.at[k]).wait()
    pltpu.make_async_copy(tails.at[planes], tails.at[planes], tsem.at[planes]).wait()
    edge = tails[planes, :, length:].astype(f32)
    hx[...] = jnp.zeros(hx.shape, f32)
    each = edge.shape[0] // (span - 1)
    for r in range(span - 1):
        row = 8 - (span - 1) + r
        for i in range(each):
            at = r * each + i
            hx[row : row + 1, i * LANES : (i + 1) * LANES] = edge[at : at + 1, :]
    lane = lax.broadcasted_iota(jnp.int32, (length, LANES), 1)
    li = lax.broadcasted_iota(jnp.int32, (length, length), 0)
    si = lax.broadcasted_iota(jnp.int32, (length, length), 1)
    causal = si <= li
    tril = causal.astype(f32).astype(bf16)
    model = ws.shape[0]
    wide_lane = lax.broadcasted_iota(jnp.int32, (length, channels), 1)

    def onehot(rows, columns, test):
        source = lax.broadcasted_iota(jnp.int32, (rows, columns), 0)
        target = lax.broadcasted_iota(jnp.int32, (rows, columns), 1)
        return test(source, target).astype(f32)

    local = rate_ref.shape[1]
    best = lax.Precision.HIGHEST
    first = it * local + ib * heads
    pick = onehot(
        LANES,
        LANES,
        lambda i, j: (i % every == first + j % heads) & (i < 3 * every) & (j < 3 * heads),
    ).astype(bf16)
    pick_offset = onehot(
        tails.shape[1],
        LANES,
        lambda i, j: (i % local == ib * heads + j % heads) & (i < 3 * local) & (j < 3 * heads),
    ).astype(bf16)
    pick_rate = onehot(local, LANES, lambda i, j: (i == ib * heads + j % heads) & (j < 3 * heads))
    pick_skip = onehot(local, channels, lambda i, j: i == ib * heads + j // SSM_DIM)
    rate = -jnp.exp(jnp.broadcast_to(rate_ref[...], (8, local)))
    rate = nn(rate, pick_rate, best)[:1]
    skip = nn(jnp.broadcast_to(skip_ref[...], (8, local)), pick_skip, best)[:1]

    def mine(ref, width):
        return ref[:, pl.ds(pl.multiple_of(ib * width, width), width)].astype(f32)

    taps = jnp.concatenate(
        [mine(ci_ref, channels), mine(cw_ref, SSM_STATE), mine(cr_ref, SSM_STATE)], axis=1
    )
    for k in range(weights):
        pltpu.make_async_copy(ws_in[k], ws.at[pl.ds(0, deep), :], wsem.at[k]).wait()
    raws[0, 0:8, :] = nn(hx[...].astype(bf16), ws[:, :conv]).astype(bf16).astype(f32)

    def product(c):
        here = pl.ds(c * length, length)
        pltpu.make_async_copy(xs.at[here, :], xs.at[here, :], xsem.at[c]).wait()
        raw = nn(xs[here, :model], ws[...]).astype(bf16)
        gate_ref[here, :] = raw[:, conv:]
        raw = raw[:, :conv].astype(f32)
        raws[c, 8:, :] = raw
        if c + 1 < planes:
            raws[c + 1, 0:8, :] = raw[length - 8 :, :]

    def chunk(c):
        here = pl.ds(c * length, length)
        total = jnp.zeros((length, raws.shape[2]), f32)
        for k in range(span):
            total = total + taps[k : k + 1, :] * raws[c, pl.ds(8 - span + 1 + k, length), :]
        mixed_in = jax.nn.silu(total).astype(bf16)
        head = mixed_in[:, :channels].astype(f32)
        write = mixed_in[:, channels : channels + SSM_STATE]
        read = mixed_in[:, channels + SSM_STATE :]
        reads_ref[here, :] = read
        step = nn(xs[here, model:], pick)
        offset = tn(tails[ib ^ c][:, :length], pick_offset)
        decay = rate * step + offset
        high = decay.astype(bf16)
        rest = decay - high.astype(f32)
        middle = rest.astype(bf16)
        least = rest - middle.astype(f32)
        split = jnp.where(lane < heads, high.astype(f32), middle.astype(f32))
        split = jnp.where(lane < 2 * heads, split, least).astype(bf16)
        running = nn(tril, split)
        running = (
            running
            + pltpu.roll(running, LANES - heads, 1)
            + pltpu.roll(running, LANES - 2 * heads, 1)
        )
        run_ref[here, :] = running + base_s[...]
        base_s[...] = base_s[...] + running[length - 1 :, :]
        across = running.T
        stepped = head * wide_heads(step, heads, lane)
        inner = nt(read, write)
        reach = jnp.exp(wide_heads(running, heads, lane))
        out = nn(read, state_s[...].astype(bf16)) * reach + skip * head
        for h in range(heads):
            spread = running[:, h : h + 1] - across[h : h + 1, :]
            fading = jnp.exp(jnp.where(causal, spread, floor_score))
            mine = (wide_lane >= h * SSM_DIM) & (wide_lane < (h + 1) * SSM_DIM)
            out = out + nn(
                (inner * fading).astype(bf16), jnp.where(mine, stepped, 0.0).astype(bf16)
            )
        mixed_ref[here, :] = out
        ending = running[length - 1 :, :]
        to_end = jnp.exp(wide_heads(ending - running, heads, lane))
        update = tn(write, (stepped * to_end).astype(bf16))
        state_s[...] = state_s[...] * reach[length - 1 :, :] + update

    for c in range(planes):
        product(c)
        chunk(c)
    state_ref[: SSM_STATE, :] = state_s[...].astype(bf16)
    total = wide_heads(base_s[...], heads, lane[:1])
    high = total.astype(bf16)
    rest = total - high.astype(f32)
    middle = rest.astype(bf16)
    least = (rest - middle.astype(f32)).astype(bf16)
    tail = jnp.concatenate(
        [high, middle, least, jnp.zeros((SSM_STATE // 8 - 3, channels), bf16)], axis=0
    )
    state_ref[SSM_STATE :, :] = tail


def finish_kernel(
    where_ref, states_ref, mixed_ref, reads_ref, gate_ref, run_ref, gain_ref, out_ref, into_s, *, heads
):
    here = where_ref[0]
    rows = mixed_ref.shape[0]
    channels = mixed_ref.shape[1]

    @pl.when(pl.program_id(0) == 0)
    def _():
        into_s[...] = jnp.zeros(into_s.shape, f32)

        def add(j, carry):
            piece = states_ref[here ^ j].astype(f32)
            decay = jnp.exp(
                piece[SSM_STATE : SSM_STATE + 1]
                + piece[SSM_STATE + 1 : SSM_STATE + 2]
                + piece[SSM_STATE + 2 : SSM_STATE + 3]
            )
            into_s[...] = into_s[...] * decay + piece[:SSM_STATE]
            return carry

        lax.fori_loop(0, here, add, 0)

    lane = lax.broadcasted_iota(jnp.int32, (rows, LANES), 1)
    reach = jnp.exp(wide_heads(run_ref[...], heads, lane))
    mixed = mixed_ref[...] + nn(reads_ref[...], into_s[...].astype(bf16)) * reach
    gated = mixed * jax.nn.silu(gate_ref[...].astype(f32))
    scale = lax.rsqrt(jnp.mean(gated * gated, axis=-1, keepdims=True) + eps)
    gain = gain_ref[:, pl.ds(pl.multiple_of(where_ref[1] * channels, channels), channels)]
    out_ref[...] = (gated * scale * gain).astype(bf16)


def params():
    return pltpu.CompilerParams(vmem_limit_bytes=60 * 1024 * 1024)


def cost(flops):
    return pl.CostEstimate(flops=flops, bytes_accessed=flops // 1000, transcendentals=0)


def shape(dims, kind):
    return jax.ShapeDtypeStruct(dims, kind)


def shards(
    tokens,
    mix_gain,
    query_proj,
    compressed_projection,
    compressed_norm_gain,
    rope_proj,
    key_up,
    value_up_weight,
    scan_input,
    scan_gate,
    scan_write,
    scan_read,
    step_proj,
    conv_input,
    conv_write,
    conv_read,
    decay_log,
    decay_offset,
    skip_gain,
    group_gain,
):
    A, B, T = lax.axis_size("a"), lax.axis_size("b"), lax.axis_size("tp")
    ia, ib, it = (lax.axis_index(name).astype(jnp.int32) for name in ("a", "b", "tp"))
    where = jnp.stack([ia, ib, it])
    rows, model = tokens.shape
    length = rows * T
    heads = key_up.shape[1] // UNROTATED_WIDTH
    key_width = key_up.shape[0] + 2 * ROPE
    groups = scan_write.shape[1] // SSM_STATE
    local = decay_log.shape[0]
    per_group = local // groups
    channels = per_group * SSM_DIM
    every = step_proj.shape[1]
    taps = conv_input.shape[0]
    span = B * length
    assert groups == B and channels == length
    assert 3 * every <= LANES and 3 * per_group <= 16
    assert length + LANES == key_width and 3 * local <= (taps - 1) * model // LANES

    def regrouped(pieces):
        moved = []
        for k in range(B):
            group = ib ^ k
            parts = [
                lax.dynamic_slice_in_dim(piece, group * width, width, 1)
                for piece, width in pieces
            ]
            value = parts[0] if len(parts) == 1 else jnp.concatenate(parts, axis=1)
            moved.append(across(value, "b", k) if k else value)
        return moved

    positions = (ia * B + ib) * length + jnp.arange(length, dtype=jnp.int32)
    half = ROPE // 2
    freqs = theta ** (-jnp.arange(half, dtype=f32) * 2.0 / ROPE)
    angle = positions.astype(f32)[:, None] * jnp.tile(freqs, LANES // half)[None, :]
    sign = jnp.where(jnp.arange(LANES) % ROPE < half, -1.0, 1.0).astype(f32)
    cosine = jnp.cos(angle)
    sine = jnp.sin(angle) * sign[None, :]

    own, key_own, edge = pl.pallas_call(
        prologue_kernel,
        in_specs=[smem()] + [vmem()] * 8,
        out_shape=(
            shape((rows, model + LANES), bf16),
            shape((rows, key_width), bf16),
            shape((8, model), bf16),
        ),
        compiler_params=params(),
        cost_estimate=cost(2 * rows * model * 1024),
        name="prologue",
    )(
        where,
        tokens,
        mix_gain.reshape(1, -1),
        compressed_projection,
        compressed_norm_gain.reshape(1, -1),
        rope_proj.T,
        step_proj.T,
        cosine,
        sine,
    )
    scan_input, key_own = lax.optimization_barrier((scan_input, key_own))
    packed = regrouped(
        [
            (scan_input, channels),
            (scan_write, SSM_STATE),
            (scan_read, SSM_STATE),
            (scan_gate, channels),
        ],
    )
    packed = jnp.concatenate(packed, axis=0)

    edge = lax.ppermute(edge, "a", [(i, i + 1) for i in range(A - 1)])
    edge = edge[8 - taps + 1 :].reshape(-1, LANES)
    offsets = three_parts(decay_offset.T).reshape(3 * local, length)
    offsets = jnp.pad(offsets, ((0, edge.shape[0] - 3 * local), (0, 0)))
    tail = jnp.concatenate([offsets, edge], axis=1)
    key_stack = jnp.concatenate(exchange(key_own, "a") + [tail], axis=0)
    packed, key_stack = lax.optimization_barrier((packed, key_stack))
    w_pieces = ring(packed, "a")
    key_pieces = []
    if B == 4:
        kside, kfront = across(key_stack, "b", 1), across(key_stack, "b", 2)
        cut = key_stack.shape[0] // 2
        kfar = jnp.concatenate([across(kside[:cut], "b", 2), across(kfront[cut:], "b", 1)], axis=0)
        key_planes = [key_stack, kside, kfront, kfar]
    else:
        key_planes = exchange(key_stack, "b")
    for piece in key_planes:
        key_pieces += exchange(piece, "tp")

    plane = [(k, 0, piece) for k, piece in enumerate(exchange(own, "b"))]
    x_pieces = []
    parts = []
    for k, start, piece in plane:
        for t, part in enumerate(exchange(piece, "tp")):
            x_pieces.append(part)
            parts.append((k, t, start, part.shape[0]))

    value_t = value_up_weight.T

    even = heads + heads % 2
    wq = query_proj
    if even != heads:
        wq = jnp.pad(wq, ((0, 0), (0, UNROTATED_WIDTH + ROPE)))
    plain, turned = pl.pallas_call(
        functools.partial(query_kernel, count=T, heads=even),
        in_specs=[smem()] + [vmem()] * (T + 3),
        out_shape=(shape((length, even * LANES), bf16), shape((length, even // 2 * LANES), bf16)),
        compiler_params=params(),
        cost_estimate=cost(2 * length * model * even * 256),
        name="query",
    )(where, *x_pieces[:T], wq, cosine, sine)

    def attend(place, lower, upper, carry):
        final = upper == A * B
        carried = (
            shape((heads, 1, length), f32),
            shape((heads, 1, length), f32),
            shape((heads, VALUE_WIDTH, length), f32),
        )
        outs = (shape((length, heads * VALUE_WIDTH), bf16),) if final else carried
        scratch = [pltpu.VMEM(c.shape, f32) for c in carried] if final else []
        return pl.pallas_call(
            functools.partial(
                attention_kernel,
                planes=B,
                cores=T,
                slots=A,
                heads=heads,
                lower=lower,
                upper=upper,
                final=final,
            ),
            in_specs=[smem()] + [vmem()] * 4 + [hbm()] * (B * T) + [vmem()] * len(carry),
            out_specs=tuple(vmem() for _ in outs),
            out_shape=outs,
            scratch_shapes=scratch
            + [
                pltpu.VMEM(((upper - lower) * length, key_width), bf16),
                pltpu.VMEM((heads, length, 2 * LANES), bf16),
                pltpu.SemaphoreType.DMA((upper - lower,)),
            ],
            compiler_params=params(),
            cost_estimate=cost(4 * length * (upper - lower) * length * LANES * 8),
            name="attention",
        )(place, plain, turned, key_up, value_t, *key_pieces, *carry)

    first_part = (3 * A * B) // 4
    carry = attend(where, 0, first_part, ())
    then, carry = lax.optimization_barrier((where, carry))

    conv = channels + 2 * SSM_STATE
    mixed, reads, gate, run, state = pl.pallas_call(
        functools.partial(
            scan_kernel,
            parts=tuple(parts),
            planes=B,
            cores=T,
            weights=A,
            length=length,
            heads=per_group,
            every=every,
        ),
        in_specs=[smem()] + [hbm()] * (len(parts) + A + B * T) + [vmem()] * 5,
        out_specs=[vmem()] * 5,
        out_shape=(
            shape((span, channels), f32),
            shape((span, SSM_STATE), bf16),
            shape((span, channels), bf16),
            shape((span, LANES), f32),
            shape((SSM_STATE + SSM_STATE // 8, channels), bf16),
        ),
        scratch_shapes=[
            pltpu.VMEM((span, model + LANES), bf16),
            pltpu.VMEM((model, conv + channels), bf16),
            pltpu.VMEM((8, model), f32),
            pltpu.VMEM((B, 8 + length, conv), f32),
            pltpu.VMEM((SSM_STATE, channels), f32),
            pltpu.VMEM((1, LANES), f32),
            pltpu.SemaphoreType.DMA((B,)),
            pltpu.SemaphoreType.DMA((A,)),
            pltpu.VMEM((B + 1,) + tail.shape, bf16),
            pltpu.SemaphoreType.DMA((B + 1,)),
        ],
        compiler_params=params(),
        cost_estimate=cost(4 * span * model * conv),
        name="state_scan",
    )(
        then,
        *x_pieces,
        *w_pieces,
        *key_pieces,
        conv_input,
        conv_write,
        conv_read,
        decay_log.reshape(1, -1),
        skip_gain.reshape(1, -1),
    )

    states = jnp.stack(exchange(state, "a"))
    then, mixed = lax.optimization_barrier((then, mixed))
    (attended,) = attend(then, first_part, A * B, carry)
    gate, attended = lax.optimization_barrier((gate, attended))

    scanned = pl.pallas_call(
        functools.partial(finish_kernel, heads=per_group),
        grid=(B,),
        in_specs=[
            smem(),
            pl.BlockSpec(states.shape, lambda i: (0, 0, 0)),
            pl.BlockSpec((length, channels), lambda i: (i, 0)),
            pl.BlockSpec((length, SSM_STATE), lambda i: (i, 0)),
            pl.BlockSpec((length, channels), lambda i: (i, 0)),
            pl.BlockSpec((length, LANES), lambda i: (i, 0)),
            pl.BlockSpec((1, group_gain.shape[0]), lambda i: (0, 0)),
        ],
        out_specs=pl.BlockSpec((length, channels), lambda i: (i, 0)),
        out_shape=shape((span, channels), bf16),
        scratch_shapes=[pltpu.VMEM((SSM_STATE, channels), f32)],
        compiler_params=params(),
        name="finish",
    )(where, states, mixed, reads, gate, run, group_gain.reshape(1, -1))
    if B > 1:
        scanned = lax.all_to_all(scanned.reshape(B, length, channels), "b", 0, 0, tiled=True)
        scanned = jnp.transpose(scanned, (1, 0, 2)).reshape(length, B * channels)
    return (attended, scanned)


def solution(mesh):
    S, T = mesh.shape["sp"], mesh.shape["tp"]
    sp = ("a", "b")
    in_specs = (
        P(("a", "b", "tp"), None),
        P(),
        P(None, "tp"),
        P(),
        P(),
        P(),
        P(None, "tp"),
        P(None, "tp"),
        P(sp, "tp"),
        P(sp, "tp"),
        P(sp, "tp"),
        P(sp, "tp"),
        P(),
        P(None, "tp"),
        P(None, "tp"),
        P(None, "tp"),
        P("tp"),
        P(sp, "tp"),
        P("tp"),
        P("tp"),
    )
    out_specs = (P(sp, "tp"), P(sp, "tp"))

    def run(*arrays):
        B = arrays[10].shape[1] // SSM_STATE // T
        assert S % B == 0
        fine = Mesh(mesh.devices.reshape(S // B, B, T), ("a", "b", "tp"))
        body = jax.shard_map(
            shards, mesh=fine, in_specs=in_specs, out_specs=out_specs, check_vma=False
        )
        return body(*arrays)

    return run
```

```python
import functools
import math

import jax
import jax.numpy as jnp
from jax import lax
from jax.experimental import pallas as pl
from jax.experimental.pallas import tpu as pltpu
from jax.sharding import Mesh
from jax.sharding import PartitionSpec as P


UNROTATED_WIDTH = 128
ROPE = 64
VALUE_WIDTH = 128
SSM_DIM = 64
SSM_STATE = 128

eps = 1e-06
theta = 10000.0
floor_score = -1e30
LANES = 128
DIRECT = 8


f32 = jnp.float32
bf16 = jnp.bfloat16


def vmem():
    return pl.BlockSpec(memory_space=pltpu.VMEM)


def smem():
    return pl.BlockSpec(memory_space=pltpu.SMEM)


def hbm():
    return pl.BlockSpec(memory_space=pl.ANY)


def nt(a, b):
    return lax.dot_general(a, b, (((1,), (1,)), ((), ())), preferred_element_type=f32)


def tn(a, b):
    return lax.dot_general(a, b, (((0,), (0,)), ((), ())), preferred_element_type=f32)


def nn(a, b, precision=None):
    return lax.dot_general(
        a, b, (((1,), (0,)), ((), ())), precision=precision, preferred_element_type=f32
    )


def exchange(value, axis):
    count = lax.axis_size(axis)
    if count == 1:
        return [value]
    assert count & (count - 1) == 0
    if count <= DIRECT:
        return [value] + [across(value, axis, k) for k in range(1, count)]
    everything = lax.all_gather(value, axis)
    here = lax.axis_index(axis)
    return [
        lax.dynamic_index_in_dim(everything, here ^ k, 0, keepdims=False) for k in range(count)
    ]


def across(value, axis, k):
    count = lax.axis_size(axis)
    return lax.ppermute(value, axis, [(i, i ^ k) for i in range(count)])


def ring(value, axis):
    count = lax.axis_size(axis)
    if count <= DIRECT:
        pieces = [value] + [None] * (count - 1)
        for way, steps in ((1, count // 2), (-1, (count - 1) // 2)):
            moving = value
            for step in range(1, steps + 1):
                place = way * step % count
                pairs = [(i, (i + way) % count) for i in range(count)]
                moving = lax.ppermute(moving, axis, pairs)
                pieces[place] = moving
        return pieces
    everything = lax.all_gather(value, axis)
    here = lax.axis_index(axis)
    return [
        lax.dynamic_index_in_dim(everything, (here - k) % count, 0, keepdims=False)
        for k in range(count)
    ]


def three_parts(values):
    high = lax.reduce_precision(values, 8, 7)
    rest = values - high
    middle = lax.reduce_precision(rest, 8, 7)
    return jnp.stack([high, middle, rest - middle]).astype(bf16)


def prologue_kernel(
    where_ref, tokens_ref, mix_ref, proj_ref, gain_ref, rope_ref, step_ref, cos_ref, sin_ref, rows_ref, key_ref, edge_ref
):
    tokens = tokens_ref[...].astype(f32)
    scale = lax.rsqrt(jnp.mean(tokens * tokens, axis=-1, keepdims=True) + eps)
    x = (tokens * scale * mix_ref[...]).astype(bf16)
    model = x.shape[1]
    rows_ref[:, :model] = x
    edge_ref[...] = x[x.shape[0] - edge_ref.shape[0] :, :]
    wide = nn(x, proj_ref[...])
    scale = lax.rsqrt(jnp.mean(wide * wide, axis=-1, keepdims=True) + eps)
    width = wide.shape[1]
    key_ref[:, :width] = (wide * scale * gain_ref[...]).astype(bf16)
    turn = nt(x, rope_ref[...])
    rope = turn.shape[1]
    half = rope // 2
    row = lax.broadcasted_iota(jnp.int32, (rope, 2 * rope), 0)
    col = lax.broadcasted_iota(jnp.int32, (rope, 2 * rope), 1) % rope
    same = (row == col).astype(f32)
    swap = (row == (col + half) % rope).astype(f32)
    best = lax.Precision.HIGHEST
    count = x.shape[0]
    here = pl.ds(pl.multiple_of(where_ref[2] * count, count), count)
    turned = nn(turn, same, best) * cos_ref[here, :] + nn(turn, swap, best) * sin_ref[here, :]
    key_ref[:, width:] = turned.astype(bf16)
    step = jax.nn.softplus(nt(x, step_ref[...]))
    count = step.shape[1]
    row = lax.broadcasted_iota(jnp.int32, (count, LANES), 0)
    col = lax.broadcasted_iota(jnp.int32, (count, LANES), 1)
    tail = jnp.zeros((x.shape[0], LANES), f32)
    for part in range(3):
        piece = step.astype(bf16)
        step = step - piece.astype(f32)
        tail = tail + nn(piece, (col == row + part * count).astype(f32).astype(bf16))
    rows_ref[:, model:] = tail.astype(bf16)


def query_kernel(where_ref, *refs, count, heads):
    pieces = refs[:count]
    w_ref, cos_ref, sin_ref, plain_ref, turned_ref = refs[count:]
    rows = pieces[0].shape[0]
    w = w_ref[...]
    lane = lax.broadcasted_iota(jnp.int32, (rows, LANES), 1)
    low = lane < ROPE
    first = lane % ROPE < ROPE // 2
    for k in range(count):
        start = pl.multiple_of((where_ref[2] ^ k) * rows, rows)
        here = pl.ds(start, rows)
        q = nn(pieces[k][:, : w.shape[0]], w).astype(bf16).astype(f32)
        cos = cos_ref[here, :]
        sin = sin_ref[here, :]
        for pair in range(heads // 2):
            base = pair * 3 * LANES
            t0 = q[:, base : base + LANES]
            t1 = q[:, base + LANES : base + 2 * LANES]
            t2 = q[:, base + 2 * LANES : base + 3 * LANES]
            odd = jnp.where(low, pltpu.roll(t1, ROPE, 1), pltpu.roll(t2, ROPE, 1))
            turn = jnp.where(low, t1, t2)
            other = jnp.where(
                first, pltpu.roll(turn, LANES - ROPE // 2, 1), pltpu.roll(turn, ROPE // 2, 1)
            )
            turned = turn * cos + other * sin
            at = pair * 2 * LANES
            plain_ref[here, at : at + LANES] = t0.astype(bf16)
            plain_ref[here, at + LANES : at + 2 * LANES] = odd.astype(bf16)
            turned_ref[here, pair * LANES : (pair + 1) * LANES] = turned.astype(bf16)


def attention_kernel(
    where_ref,
    plain_ref,
    turned_ref,
    ku_ref,
    vu_ref,
    *refs,
    planes,
    cores,
    slots,
    heads,
    lower,
    upper,
    final,
):
    arrays = planes * cores
    pieces = refs[:arrays]
    refs = refs[arrays:]
    if lower > 0:
        before, refs = refs[:3], refs[3:]
    if final:
        out_ref, top_s, sum_s, acc_s, keys, q_s, sems = refs
    else:
        top_s, sum_s, acc_s, keys, q_s, sems = refs
    length = plain_ref.shape[0]
    rows = length // cores
    width = ku_ref.shape[0]
    ia, ib, it = where_ref[0], where_ref[1], where_ref[2]
    here = ia * planes + ib
    last = jnp.minimum(here + 1, upper)
    factor = (UNROTATED_WIDTH + ROPE) ** -0.5 * math.log2(math.e)

    for k in range(planes):
        for t in range(cores):
            for z in range(slots):
                block = (ia ^ z) * planes + (ib ^ k)

                @pl.when((block >= lower) & (block < last))
                def _():
                    start = pl.multiple_of((block - lower) * length + (it ^ t) * rows, rows)
                    pltpu.make_async_copy(
                        pieces[k * cores + t].at[pl.ds(z * rows, rows), :],
                        keys.at[pl.ds(start, rows), :],
                        sems.at[block - lower],
                    ).start()

    lane = lax.broadcasted_iota(jnp.int32, (length, LANES), 1)
    for h in range(heads):
        q_s[h, :, :LANES] = plain_ref[:, h * LANES : (h + 1) * LANES]
        turned = turned_ref[:, (h // 2) * LANES : (h // 2 + 1) * LANES]
        keep = lane < ROPE if h % 2 == 0 else lane >= ROPE
        q_s[h, :, LANES:] = jnp.where(keep, turned, jnp.zeros_like(turned))
    if lower > 0:
        top_s[...] = before[0][...]
        sum_s[...] = before[1][...]
        acc_s[...] = before[2][...]
    else:
        top_s[...] = jnp.full(top_s.shape, floor_score, f32)
        sum_s[...] = jnp.zeros(sum_s.shape, f32)
        acc_s[...] = jnp.zeros(acc_s.shape, f32)

    def visit(block, masked):
        at = pl.ds(pl.multiple_of((block - lower) * length, length), length)
        pltpu.make_async_copy(keys.at[at, :], keys.at[at, :], sems.at[block - lower]).wait()
        latent = keys[at, :width]
        shared = keys[at, width:]
        key_plain = nn(latent, ku_ref[...]).astype(bf16)
        values = nt(vu_ref[...], latent).astype(bf16)
        if masked:
            key_at = lax.broadcasted_iota(jnp.int32, (length, length), 0)
            query_at = lax.broadcasted_iota(jnp.int32, (length, length), 1)
            seen = key_at <= query_at
        for h in range(heads):
            key = jnp.concatenate([key_plain[:, h * LANES : (h + 1) * LANES], shared], axis=1)
            score = nt(key, q_s[h])
            if masked:
                score = jnp.where(seen, score, -jnp.inf)
            old = top_s[h]
            top = jnp.maximum(old, jnp.max(score, axis=0, keepdims=True))
            weight = jnp.exp2((score - top) * factor)
            shrink = jnp.exp2((old - top) * factor)
            top_s[h] = top
            sum_s[h] = sum_s[h] * shrink + jnp.sum(weight, axis=0, keepdims=True)
            acc_s[h] = acc_s[h] * shrink + nn(
                values[h * VALUE_WIDTH : (h + 1) * VALUE_WIDTH, :], weight.astype(bf16)
            )

    def body(block, carry):
        visit(block, False)
        return carry

    lax.fori_loop(lower, jnp.minimum(here, upper), body, 0)

    @pl.when((here >= lower) & (here < upper))
    def _():
        visit(here, True)

    if final:
        for h in range(heads):
            result = (acc_s[h] / sum_s[h]).T
            out_ref[:, h * VALUE_WIDTH : (h + 1) * VALUE_WIDTH] = result.astype(bf16)


def wide_heads(values, heads, lane):
    tiles = []
    for pair in range(0, heads, 2):
        a = jnp.broadcast_to(values[:, pair : pair + 1], (values.shape[0], LANES))
        b = jnp.broadcast_to(values[:, pair + 1 : pair + 2], (values.shape[0], LANES))
        tiles.append(jnp.where(lane < SSM_DIM, a, b))
    return jnp.concatenate(tiles, axis=1)


def row_copies(where_ref, pieces, parts, target, sems, length, cores, width):
    ib, it = where_ref[1], where_ref[2]
    rows = length // cores
    for piece, (k, t, start, count) in zip(pieces, parts):
        block = ib ^ k
        at = pl.multiple_of(block * length + (it ^ t) * rows + start, count)
        yield pltpu.make_async_copy(
            piece.at[:, pl.ds(0, width)], target.at[pl.ds(at, count), :], sems.at[block]
        )


def weight_copies(where_ref, piece, plane, target, sem, planes):
    depth = piece.shape[0] // planes
    for k in range(planes):
        at = pl.multiple_of((plane * planes + (where_ref[1] ^ k)) * depth, depth)
        yield pltpu.make_async_copy(
            piece.at[pl.ds(k * depth, depth), :], target.at[pl.ds(at, depth), :], sem
        )


def scan_kernel(
    where_ref,
    *refs,
    parts,
    planes,
    cores,
    weights,
    length,
    heads,
    every,
):
    nx = len(parts)
    xs_in = refs[:nx]
    ws_in = refs[nx : nx + weights]
    tails_in = refs[nx + weights : nx + weights + planes * cores]
    (
        ci_ref,
        cw_ref,
        cr_ref,
        rate_ref,
        skip_ref,
        mixed_ref,
        reads_ref,
        run_ref,
        state_ref,
        xs,
        ws,
        hx,
        raws,
        state_s,
        base_s,
        xsem,
        wsem,
        tails,
        tsem,
    ) = refs[nx + weights + planes * cores :]
    ia, ib, it = where_ref[0], where_ref[1], where_ref[2]
    deep = ws_in[0].shape[0]
    channels = heads * SSM_DIM
    span = ci_ref.shape[0]
    bottom = tails_in[0].shape[0] - tails.shape[1]
    for k in range(planes):
        for t in range(cores):
            piece = tails_in[k * cores + t].at[pl.ds(bottom, tails.shape[1]), :]
            if t == 0:
                pltpu.make_async_copy(piece, tails.at[k], tsem.at[k]).start()

            @pl.when(((ib ^ k) == planes - 1) & ((it ^ t) == cores - 1))
            def _():
                pltpu.make_async_copy(piece, tails.at[planes], tsem.at[planes]).start()

    for k in range(weights):
        for copy in weight_copies(
            where_ref, ws_in[k], (ia - k + weights) % weights, ws, wsem.at[k], planes
        ):
            copy.start()
    for copy in row_copies(where_ref, xs_in, parts, xs, xsem, length, cores, xs.shape[1]):
        copy.start()
    state_s[...] = jnp.zeros(state_s.shape, f32)
    base_s[...] = jnp.zeros(base_s.shape, f32)
    for k in range(planes):
        pltpu.make_async_copy(tails.at[k], tails.at[k], tsem.at[k]).wait()
    pltpu.make_async_copy(tails.at[planes], tails.at[planes], tsem.at[planes]).wait()
    edge = tails[planes, :, length:].astype(f32)
    edge = jnp.where(ia > 0, edge, jnp.zeros_like(edge))
    hx[...] = jnp.zeros(hx.shape, f32)
    each = edge.shape[0] // (span - 1)
    for r in range(span - 1):
        row = 8 - (span - 1) + r
        for i in range(each):
            at = r * each + i
            hx[row : row + 1, i * LANES : (i + 1) * LANES] = edge[at : at + 1, :]
    lane = lax.broadcasted_iota(jnp.int32, (length, LANES), 1)
    li = lax.broadcasted_iota(jnp.int32, (length, length), 0)
    si = lax.broadcasted_iota(jnp.int32, (length, length), 1)
    causal = si <= li
    tril = causal.astype(f32).astype(bf16)
    model = ws.shape[0]
    wide_lane = lax.broadcasted_iota(jnp.int32, (length, channels), 1)

    def onehot(rows, columns, test):
        source = lax.broadcasted_iota(jnp.int32, (rows, columns), 0)
        target = lax.broadcasted_iota(jnp.int32, (rows, columns), 1)
        return test(source, target).astype(f32)

    local = rate_ref.shape[1]
    best = lax.Precision.HIGHEST
    first = it * local + ib * heads
    pick = onehot(
        LANES,
        LANES,
        lambda i, j: (i % every == first + j % heads) & (i < 3 * every) & (j < 3 * heads),
    ).astype(bf16)
    pick_offset = onehot(
        tails.shape[1],
        LANES,
        lambda i, j: (i % local == ib * heads + j % heads) & (i < 3 * local) & (j < 3 * heads),
    ).astype(bf16)
    pick_rate = onehot(local, LANES, lambda i, j: (i == ib * heads + j % heads) & (j < 3 * heads))
    pick_skip = onehot(local, channels, lambda i, j: i == ib * heads + j // SSM_DIM)
    rate = -jnp.exp(jnp.broadcast_to(rate_ref[...], (8, local)))
    rate = nn(rate, pick_rate, best)[:1]
    skip = nn(jnp.broadcast_to(skip_ref[...], (8, local)), pick_skip, best)[:1]

    def mine(ref, width):
        return ref[:, pl.ds(pl.multiple_of(ib * width, width), width)].astype(f32)

    taps = jnp.concatenate(
        [mine(ci_ref, channels), mine(cw_ref, SSM_STATE), mine(cr_ref, SSM_STATE)], axis=1
    )
    for k in range(weights):
        pltpu.make_async_copy(ws_in[k], ws.at[pl.ds(0, deep), :], wsem.at[k]).wait()
    raws[0, 0:8, :] = nn(hx[...].astype(bf16), ws[...]).astype(bf16).astype(f32)

    def product(c):
        here = pl.ds(c * length, length)
        pltpu.make_async_copy(xs.at[here, :], xs.at[here, :], xsem.at[c]).wait()
        raw = nn(xs[here, :model], ws[...]).astype(bf16)
        raw = raw.astype(f32)
        raws[c, 8:, :] = raw
        if c + 1 < planes:
            raws[c + 1, 0:8, :] = raw[length - 8 :, :]

    def chunk(c):
        here = pl.ds(c * length, length)
        total = jnp.zeros((length, raws.shape[2]), f32)
        for k in range(span):
            total = total + taps[k : k + 1, :] * raws[c, pl.ds(8 - span + 1 + k, length), :]
        mixed_in = jax.nn.silu(total).astype(bf16)
        head = mixed_in[:, :channels].astype(f32)
        write = mixed_in[:, channels : channels + SSM_STATE]
        read = mixed_in[:, channels + SSM_STATE :]
        reads_ref[here, :] = read
        step = nn(xs[here, model:], pick)
        offset = tn(tails[ib ^ c][:, :length], pick_offset)
        decay = rate * step + offset
        high = decay.astype(bf16)
        rest = decay - high.astype(f32)
        middle = rest.astype(bf16)
        least = rest - middle.astype(f32)
        split = jnp.where(lane < heads, high.astype(f32), middle.astype(f32))
        split = jnp.where(lane < 2 * heads, split, least).astype(bf16)
        running = nn(tril, split)
        running = (
            running
            + pltpu.roll(running, LANES - heads, 1)
            + pltpu.roll(running, LANES - 2 * heads, 1)
        )
        run_ref[here, :] = running + base_s[...]
        base_s[...] = base_s[...] + running[length - 1 :, :]
        across = running.T
        stepped = head * wide_heads(step, heads, lane)
        inner = nt(read, write)
        reach = jnp.exp(wide_heads(running, heads, lane))
        out = nn(read, state_s[...].astype(bf16)) * reach + skip * head
        for h in range(heads):
            spread = running[:, h : h + 1] - across[h : h + 1, :]
            fading = jnp.exp(jnp.where(causal, spread, floor_score))
            mine = (wide_lane >= h * SSM_DIM) & (wide_lane < (h + 1) * SSM_DIM)
            out = out + nn(
                (inner * fading).astype(bf16), jnp.where(mine, stepped, 0.0).astype(bf16)
            )
        mixed_ref[here, :] = out
        ending = running[length - 1 :, :]
        to_end = jnp.exp(wide_heads(ending - running, heads, lane))
        update = tn(write, (stepped * to_end).astype(bf16))
        state_s[...] = state_s[...] * reach[length - 1 :, :] + update

    for c in range(planes):
        product(c)
        chunk(c)
    state_ref[: SSM_STATE, :] = state_s[...].astype(bf16)
    total = wide_heads(base_s[...], heads, lane[:1])
    high = total.astype(bf16)
    rest = total - high.astype(f32)
    middle = rest.astype(bf16)
    least = (rest - middle.astype(f32)).astype(bf16)
    tail = jnp.concatenate(
        [high, middle, least, jnp.zeros((SSM_STATE // 8 - 3, channels), bf16)], axis=0
    )
    state_ref[SSM_STATE :, :] = tail


def gate_kernel(where_ref, *refs, parts, planes, cores, weights, length):
    nx = len(parts)
    xs_in = refs[:nx]
    ws_in = refs[nx : nx + weights]
    out_ref, xs, ws, xsem, wsem = refs[nx + weights :]
    ia = where_ref[0]
    deep = ws_in[0].shape[0]
    model = ws.shape[0]

    for k in range(weights):
        for copy in weight_copies(
            where_ref, ws_in[k], ia ^ k, ws, wsem.at[k], planes
        ):
            copy.start()
    for copy in row_copies(where_ref, xs_in, parts, xs, xsem, length, cores, model):
        copy.start()
    for k in range(weights):
        pltpu.make_async_copy(ws_in[k], ws.at[pl.ds(0, deep), :], wsem.at[k]).wait()
    batch = 2 if planes % 2 == 0 else 1

    def some(c, carry):
        for i in range(batch):
            block = c * batch + i
            at = pl.ds(pl.multiple_of(block * length, length), length)
            pltpu.make_async_copy(xs.at[at, :], xs.at[at, :], xsem.at[block]).wait()
        here = pl.ds(pl.multiple_of(c * batch * length, batch * length), batch * length)
        out_ref[here, :] = nn(xs[here, :], ws[...]).astype(bf16)
        return carry

    lax.fori_loop(0, planes // batch, some, 0)


def finish_kernel(where_ref, *refs, heads, planes):
    states, refs = refs[: len(refs) - 7], refs[len(refs) - 7 :]
    mixed_ref, reads_ref, gate_ref, run_ref, gain_ref, out_ref, into_s = refs
    here = where_ref[0]
    rows = mixed_ref.shape[0]
    channels = mixed_ref.shape[1]

    @pl.when(pl.program_id(0) == 0)
    def _():
        into_s[...] = jnp.zeros(into_s.shape, f32)

        def add(piece):
            piece = piece.astype(f32)
            total = piece[SSM_STATE : SSM_STATE + 3].sum(axis=0, keepdims=True)
            into_s[...] = into_s[...] * jnp.exp(total) + piece[:SSM_STATE]

        def stacked(j, carry):
            add(states[0][here ^ j])
            return carry

        if len(states) == 1:
            lax.fori_loop(0, here, stacked, 0)
        else:
            for j in range(planes - 1):
                for k in range(planes):

                    @pl.when((j < here) & ((here ^ k) == j))
                    def _():
                        add(states[k][...])

    lane = lax.broadcasted_iota(jnp.int32, (rows, LANES), 1)
    reach = jnp.exp(wide_heads(run_ref[...], heads, lane))
    mixed = mixed_ref[...] + nn(reads_ref[...], into_s[...].astype(bf16)) * reach
    gated = mixed * jax.nn.silu(gate_ref[...].astype(f32))
    scale = lax.rsqrt(jnp.mean(gated * gated, axis=-1, keepdims=True) + eps)
    gain = gain_ref[:, pl.ds(pl.multiple_of(where_ref[1] * channels, channels), channels)]
    out_ref[...] = (gated * scale * gain).astype(bf16)


def params():
    return pltpu.CompilerParams(vmem_limit_bytes=60 * 1024 * 1024)


def cost(flops):
    return pl.CostEstimate(flops=flops, bytes_accessed=flops // 1000, transcendentals=0)


def shape(dims, kind):
    return jax.ShapeDtypeStruct(dims, kind)


def shards(
    tokens,
    mix_gain,
    query_proj,
    compressed_projection,
    compressed_norm_gain,
    rope_proj,
    key_up,
    value_up_weight,
    scan_input,
    scan_gate,
    scan_write,
    scan_read,
    step_proj,
    conv_input,
    conv_write,
    conv_read,
    decay_log,
    decay_offset,
    skip_gain,
    group_gain,
):
    A, B, T = lax.axis_size("a"), lax.axis_size("b"), lax.axis_size("tp")
    ia, ib, it = (lax.axis_index(name).astype(jnp.int32) for name in ("a", "b", "tp"))
    where = jnp.stack([ia, ib, it])
    rows, model = tokens.shape
    length = rows * T
    heads = key_up.shape[1] // UNROTATED_WIDTH
    key_width = key_up.shape[0] + 2 * ROPE
    groups = scan_write.shape[1] // SSM_STATE
    local = decay_log.shape[0]
    per_group = local // groups
    channels = per_group * SSM_DIM
    every = step_proj.shape[1]
    taps = conv_input.shape[0]
    span = B * length
    assert groups == B and channels == length
    assert 3 * every <= LANES and 3 * per_group <= 16
    assert length + LANES == key_width and 3 * local <= (taps - 1) * model // LANES

    def regrouped(pieces):
        moved = []
        for k in range(B):
            group = ib ^ k
            parts = [
                lax.dynamic_slice_in_dim(piece, group * width, width, 1)
                for piece, width in pieces
            ]
            value = parts[0] if len(parts) == 1 else jnp.concatenate(parts, axis=1)
            moved.append(across(value, "b", k) if k else value)
        return moved

    positions = (ia * B + ib) * length + jnp.arange(length, dtype=jnp.int32)
    half = ROPE // 2
    freqs = theta ** (-jnp.arange(half, dtype=f32) * 2.0 / ROPE)
    angle = positions.astype(f32)[:, None] * jnp.tile(freqs, LANES // half)[None, :]
    sign = jnp.where(jnp.arange(LANES) % ROPE < half, -1.0, 1.0).astype(f32)
    cosine = jnp.cos(angle)
    sine = jnp.sin(angle) * sign[None, :]

    own, key_own, edge = pl.pallas_call(
        prologue_kernel,
        in_specs=[smem()] + [vmem()] * 8,
        out_shape=(
            shape((rows, model + LANES), bf16),
            shape((rows, key_width), bf16),
            shape((8, model), bf16),
        ),
        compiler_params=params(),
        cost_estimate=cost(2 * rows * model * 1024),
        name="prologue",
    )(
        where,
        tokens,
        mix_gain.reshape(1, -1),
        compressed_projection,
        compressed_norm_gain.reshape(1, -1),
        rope_proj.T,
        step_proj.T,
        cosine,
        sine,
    )
    scan_input, key_own = lax.optimization_barrier((scan_input, key_own))
    packed = regrouped(
        [
            (scan_input, channels),
            (scan_write, SSM_STATE),
            (scan_read, SSM_STATE),
            (scan_gate, channels),
        ],
    )
    conv = channels + 2 * SSM_STATE
    gating = jnp.concatenate([piece[:, conv:] for piece in packed], axis=0)
    packed = jnp.concatenate([piece[:, :conv] for piece in packed], axis=0)

    edge = lax.ppermute(edge, "a", [(i, (i + 1) % A) for i in range(A)])
    edge = edge[8 - taps + 1 :].reshape(-1, LANES)
    offsets = three_parts(decay_offset.T).reshape(3 * local, length)
    offsets = jnp.pad(offsets, ((0, edge.shape[0] - 3 * local), (0, 0)))
    tail = jnp.concatenate([offsets, edge], axis=1)
    key_stack = jnp.concatenate(exchange(key_own, "a") + [tail], axis=0)
    packed, key_stack = lax.optimization_barrier((packed, key_stack))
    w_pieces = ring(packed, "a")
    gating, w_pieces[0] = lax.optimization_barrier((gating, w_pieces[0]))
    g_pieces = exchange(gating, "a")
    key_pieces = []
    if B == 4:
        kside, kfront = across(key_stack, "b", 1), across(key_stack, "b", 2)
        cut = key_stack.shape[0] // 2
        kfar = jnp.concatenate([across(kside[:cut], "b", 2), across(kfront[cut:], "b", 1)], axis=0)
        key_planes = [key_stack, kside, kfront, kfar]
    else:
        key_planes = exchange(key_stack, "b")
    for piece in key_planes:
        key_pieces += exchange(piece, "tp")

    plane = [(k, 0, piece) for k, piece in enumerate(exchange(own, "b"))]
    x_pieces = []
    parts = []
    for k, start, piece in plane:
        for t, part in enumerate(exchange(piece, "tp")):
            x_pieces.append(part)
            parts.append((k, t, start, part.shape[0]))

    value_t = value_up_weight.T

    even = heads + heads % 2
    wq = query_proj
    if even != heads:
        wq = jnp.pad(wq, ((0, 0), (0, UNROTATED_WIDTH + ROPE)))
    plain, turned = pl.pallas_call(
        functools.partial(query_kernel, count=T, heads=even),
        in_specs=[smem()] + [vmem()] * (T + 3),
        out_shape=(shape((length, even * LANES), bf16), shape((length, even // 2 * LANES), bf16)),
        compiler_params=params(),
        cost_estimate=cost(2 * length * model * even * 256),
        name="query",
    )(where, *x_pieces[:T], wq, cosine, sine)

    def attend(place, lower, upper, carry):
        final = upper == A * B
        carried = (
            shape((heads, 1, length), f32),
            shape((heads, 1, length), f32),
            shape((heads, VALUE_WIDTH, length), f32),
        )
        outs = (shape((length, heads * VALUE_WIDTH), bf16),) if final else carried
        scratch = [pltpu.VMEM(c.shape, f32) for c in carried] if final else []
        return pl.pallas_call(
            functools.partial(
                attention_kernel,
                planes=B,
                cores=T,
                slots=A,
                heads=heads,
                lower=lower,
                upper=upper,
                final=final,
            ),
            in_specs=[smem()] + [vmem()] * 4 + [hbm()] * (B * T) + [vmem()] * len(carry),
            out_specs=tuple(vmem() for _ in outs),
            out_shape=outs,
            scratch_shapes=scratch
            + [
                pltpu.VMEM(((upper - lower) * length, key_width), bf16),
                pltpu.VMEM((heads, length, 2 * LANES), bf16),
                pltpu.SemaphoreType.DMA((upper - lower,)),
            ],
            compiler_params=params(),
            cost_estimate=cost(4 * length * (upper - lower) * length * LANES * 8),
            name="attention",
        )(place, plain, turned, key_up, value_t, *key_pieces, *carry)

    first_part = (5 * A * B) // 8
    carry = attend(where, 0, first_part, ())
    then, carry = lax.optimization_barrier((where, carry))

    mixed, reads, run, state = pl.pallas_call(
        functools.partial(
            scan_kernel,
            parts=tuple(parts),
            planes=B,
            cores=T,
            weights=A,
            length=length,
            heads=per_group,
            every=every,
        ),
        in_specs=[smem()] + [hbm()] * (len(parts) + A + B * T) + [vmem()] * 5,
        out_specs=[vmem()] * 4,
        out_shape=(
            shape((span, channels), f32),
            shape((span, SSM_STATE), bf16),
            shape((span, LANES), f32),
            shape((SSM_STATE + SSM_STATE // 8, channels), bf16),
        ),
        scratch_shapes=[
            pltpu.VMEM((span, model + LANES), bf16),
            pltpu.VMEM((model, conv), bf16),
            pltpu.VMEM((8, model), f32),
            pltpu.VMEM((B, 8 + length, conv), f32),
            pltpu.VMEM((SSM_STATE, channels), f32),
            pltpu.VMEM((1, LANES), f32),
            pltpu.SemaphoreType.DMA((B,)),
            pltpu.SemaphoreType.DMA((A,)),
            pltpu.VMEM((B + 1,) + tail.shape, bf16),
            pltpu.SemaphoreType.DMA((B + 1,)),
        ],
        compiler_params=params(),
        cost_estimate=cost(4 * span * model * conv),
        name="state_scan",
    )(
        then,
        *x_pieces,
        *w_pieces,
        *key_pieces,
        conv_input,
        conv_write,
        conv_read,
        decay_log.reshape(1, -1),
        skip_gain.reshape(1, -1),
    )

    states = exchange(state, "a")
    if A > DIRECT:
        states = [jnp.stack(states)]
    then, mixed = lax.optimization_barrier((then, mixed))
    gate = pl.pallas_call(
        functools.partial(
            gate_kernel, parts=tuple(parts), planes=B, cores=T, weights=A, length=length
        ),
        in_specs=[smem()] + [hbm()] * (len(parts) + A),
        out_specs=vmem(),
        out_shape=shape((span, channels), bf16),
        scratch_shapes=[
            pltpu.VMEM((span, model), bf16),
            pltpu.VMEM((model, channels), bf16),
            pltpu.SemaphoreType.DMA((B,)),
            pltpu.SemaphoreType.DMA((A,)),
        ],
        compiler_params=params(),
        cost_estimate=cost(2 * span * model * channels),
        name="gate",
    )(then, *x_pieces, *g_pieces)

    scanned = pl.pallas_call(
        functools.partial(finish_kernel, heads=per_group, planes=A),
        grid=(2,),
        in_specs=[
            smem(),
            *[
                pl.BlockSpec(piece.shape, lambda i, rank=piece.ndim: (0,) * rank)
                for piece in states
            ],
            pl.BlockSpec((span // 2, channels), lambda i: (i, 0)),
            pl.BlockSpec((span // 2, SSM_STATE), lambda i: (i, 0)),
            pl.BlockSpec((span // 2, channels), lambda i: (i, 0)),
            pl.BlockSpec((span // 2, LANES), lambda i: (i, 0)),
            pl.BlockSpec((1, group_gain.shape[0]), lambda i: (0, 0)),
        ],
        out_specs=pl.BlockSpec((span // 2, channels), lambda i: (i, 0)),
        out_shape=shape((span, channels), bf16),
        scratch_shapes=[pltpu.VMEM((SSM_STATE, channels), f32)],
        compiler_params=params(),
        name="finish",
    )(where, *states, mixed, reads, gate, run, group_gain.reshape(1, -1))
    last, scanned = lax.optimization_barrier((then, scanned))
    (attended,) = attend(last, first_part, A * B, carry)
    if B > 1:
        scanned = lax.all_to_all(scanned.reshape(B, length, channels), "b", 0, 0, tiled=True)
        scanned = jnp.transpose(scanned, (1, 0, 2)).reshape(length, B * channels)
    return (attended, scanned)


def solution(mesh):
    S, T = mesh.shape["sp"], mesh.shape["tp"]
    sp = ("a", "b")
    in_specs = (
        P(("a", "b", "tp"), None),
        P(),
        P(None, "tp"),
        P(),
        P(),
        P(),
        P(None, "tp"),
        P(None, "tp"),
        P(sp, "tp"),
        P(sp, "tp"),
        P(sp, "tp"),
        P(sp, "tp"),
        P(),
        P(None, "tp"),
        P(None, "tp"),
        P(None, "tp"),
        P("tp"),
        P(sp, "tp"),
        P("tp"),
        P("tp"),
    )
    out_specs = (P(sp, "tp"), P(sp, "tp"))

    def run(*arrays):
        B = arrays[10].shape[1] // SSM_STATE // T
        assert S % B == 0
        fine = Mesh(mesh.devices.reshape(S // B, B, T), ("a", "b", "tp"))
        body = jax.shard_map(
            shards, mesh=fine, in_specs=in_specs, out_specs=out_specs, check_vma=False
        )
        return body(*arrays)

    return run
```
